256 devices in a mesh: st: 16 (over y, x), tp: 16 (over z, core).
Axes of the slice: x: 4, y: 4, z: 8, core: 2. Of those that a mesh axis runs over, the one named last changes fastest.
Arguments:
- tokens: bfloat16 [8192, 4096], P('st', 'tp'), may hold values from -6 to 6
- w_query: bfloat16 [4096, 2048], P(None, 'tp'), may hold values from -0.09375 to 0.09375
- w_key: bfloat16 [4096, 2048], P(None, 'tp'), may hold values from -0.09375 to 0.09375
- w_value: bfloat16 [4096, 4096], P(None, 'tp'), may hold values from -0.09375 to 0.09375
- w_mem_query: bfloat16 [4096, 2048], P(None, 'tp'), may hold values from -0.09375 to 0.09375
- w_mem_key: bfloat16 [4096, 2048], P(None, 'tp'), may hold values from -0.09375 to 0.09375
- w_mem_value: bfloat16 [4096, 2048], P(None, 'tp'), may hold values from -0.09375 to 0.09375
- w_gate: bfloat16 [4096, 16], P(None, 'tp'), may hold values from -0.09375 to 0.09375
- w_lift: bfloat16 [16, 128, 256], P('tp'), may hold values from -4 to 4
- decay_rate: float32 [16], P('tp'), may hold values from 0.000390625 to 0.1
- store: bfloat16 [2048, 64, 4096], P('st', None, 'tp'), may hold values from -6 to 6
- passage_ids: int32 [64, 2], P('st'), may hold values from 0 to 2047, as said below
Outputs:
- mixed: bfloat16 [8192, 4096], P('st', 'tp')
The draws below stay inside these ranges and needn't reach their ends.
Inputs may be any that keep to these rules, and one draw needn't show every extreme that they name: `passage_ids`: passage p is held by index p // 128 of st. Among the requests of the rows of one device along st, at most 1 name passages held by one index of st, and in every draw some index receives exactly 1 of them.
All inputs are finite; a program needn't handle non-finite values.
Results may differ from the reference program's by a relative error of at most 0.0095.
Values may be sent and summed in bfloat16 or wider, within the bound.
A program may use at most 64 MiB of HBM per device.

```python
import jax
import jax.numpy as jnp
from jax import lax

D = 4096
HEADS = 16
KEY_DIM = 128
VALUE_DIM = 256
MEM_DIM = 128
TOK_DEV = 512
SEQ_LEN = 512
RET_BLOCK = 64
BLOCK = 128
PICKS = 2
PASS_ROWS = 64
PASS_DEV = 128
CAP = 1
TOKENS = 8192
BLOCKS = 64
PASSAGES = 2048
N_ST = 16


def draw_decay_rate(key, part):
    pick_key, slow_key, fast_key = jax.random.split(key, 3)
    quick = jax.random.uniform(pick_key, (HEADS,)) < 0.5
    slow_rate = jnp.exp(jax.random.uniform(slow_key, (HEADS,), minval=jnp.log(0.2 / SEQ_LEN), maxval=jnp.log(2.0 / SEQ_LEN)))
    fast_rate = jnp.exp(jax.random.uniform(fast_key, (HEADS,), minval=jnp.log(0.03), maxval=jnp.log(0.1)))
    return jnp.where(quick, fast_rate, slow_rate).astype(jnp.float32)


def draw_passage_ids(key, part):
    requests = TOK_DEV // BLOCK * PICKS
    slot_count = N_ST * CAP
    owners = jnp.repeat(jnp.arange(N_ST, dtype=jnp.int32), CAP)
    copies = jnp.tile(jnp.arange(CAP, dtype=jnp.int32), N_ST)

    def one_device(device):
        device_key = jax.random.fold_in(key, device)
        rank_key, shuffle_key, first_key, second_key = jax.random.split(device_key, 4)
        before = (device + N_ST - 1) % N_ST
        across = (device + N_ST // 2) % N_ST
        priority = jnp.where(owners == before, 0, jnp.where((owners == across) & (copies == 0), 1, 2))
        noise_rank = jax.random.randint(rank_key, (slot_count,), 0, 1 << 12)
        scores = priority * (1 << 24) + noise_rank * slot_count + jnp.arange(slot_count, dtype=jnp.int32)
        chosen = owners[jnp.argsort(scores)[:requests]]
        chosen = chosen[jax.random.permutation(shuffle_key, requests)]
        first_pick = jax.random.randint(first_key, (requests,), 0, PASS_DEV)
        second_pick = jax.random.randint(second_key, (requests,), 0, PASS_DEV)
        return chosen * PASS_DEV + jnp.minimum(first_pick, second_pick)
    drawn = jax.vmap(one_device)(jnp.arange(N_ST, dtype=jnp.int32))
    return drawn.reshape(BLOCKS, PICKS).astype(jnp.int32)


def block_scale(stream_key, extent, cuts, least, top_value):
    def one(dim, shards_of):
        heights = jax.random.uniform(jax.random.fold_in(jax.random.fold_in(stream_key, 6), dim), (shards_of,), jnp.float32, least / len(cuts), top_value / len(cuts))
        return jnp.repeat(jnp.exp(heights), extent[dim] // shards_of).reshape((-1,) + (1,) * (len(extent) - dim - 1))

    factor_of = one(*cuts[0])
    for cut in cuts[1:]:
        factor_of = factor_of * one(*cut)
    return factor_of


def noise(key, dims, scale, limit, cuts=(), held_as=jnp.bfloat16):
    entries = scale * jax.random.normal(key, dims, jnp.float32)
    if cuts:
        entries = entries * block_scale(key, dims, cuts, -0.22, 0.18)
    return jnp.clip(entries, -limit, limit).astype(held_as)


def setup_inputs(seed: int = 0) -> dict:
    streams_of = jax.random.split(jax.random.key(seed), 13)
    return {
        "tokens": noise(streams_of[0], (TOKENS, D), 1.0, 6.0, ((0, 16), (1, 16))),
        "w_query": noise(streams_of[1], (D, HEADS * KEY_DIM), D ** -0.5, 0.09375, ((1, 16),)),
        "w_key": noise(streams_of[2], (D, HEADS * KEY_DIM), D ** -0.5, 0.09375, ((1, 16),)),
        "w_value": noise(streams_of[3], (D, HEADS * VALUE_DIM), D ** -0.5, 0.09375, ((1, 16),)),
        "w_mem_query": noise(streams_of[4], (D, HEADS * MEM_DIM), D ** -0.5, 0.09375, ((1, 16),)),
        "w_mem_key": noise(streams_of[5], (D, HEADS * MEM_DIM), D ** -0.5, 0.09375, ((1, 16),)),
        "w_mem_value": noise(streams_of[6], (D, HEADS * MEM_DIM), D ** -0.5, 0.09375, ((1, 16),)),
        "w_gate": noise(streams_of[7], (D, HEADS), D ** -0.5, 0.09375, ((1, 16),)),
        "w_lift": noise(streams_of[8], (HEADS, MEM_DIM, VALUE_DIM), 0.7, 4.0, ((0, 16),)),
        "decay_rate": draw_decay_rate(jax.random.fold_in(streams_of[12], 71), 0),
        "store": noise(streams_of[10], (PASSAGES, PASS_ROWS, D), 1.0, 6.0, ((0, 16), (2, 16))),
        "passage_ids": draw_passage_ids(jax.random.fold_in(streams_of[12], 71), 0),
    }


norm_eps = 1e-06
rope_base = 10000.0

def rotate(values, positions):
    half_dim = values.shape[-1] // 2
    inverse = rope_base ** (-jnp.arange(half_dim, dtype=jnp.float32) / half_dim)
    angles = positions.astype(jnp.float32)[:, None] * inverse[None, :]
    cosine = jnp.cos(angles)[:, None, :]
    sine_table = jnp.sin(angles)[:, None, :]
    first_half = values[..., :half_dim]
    second_half = values[..., half_dim:]
    return jnp.concatenate([first_half * cosine - second_half * sine_table, first_half * sine_table + second_half * cosine], axis=-1)

def head_norm(values):
    return values * lax.rsqrt(lax.optimization_barrier(jnp.mean(values * values, axis=-1, keepdims=True)) + norm_eps)

def group_norm(values):
    centred = values - lax.optimization_barrier(jnp.mean(values, axis=-1, keepdims=True))
    return centred * lax.rsqrt(lax.optimization_barrier(jnp.mean(centred * centred, axis=-1, keepdims=True)) + norm_eps)

def retention(ret_query, ret_key, ret_value, rates, block_len):
    tokens_all, head_count, key_dim = ret_query.shape
    value_dim = ret_value.shape[-1]
    sequences = tokens_all // SEQ_LEN
    block_count = SEQ_LEN // block_len

    def blocked(array):
        shaped = array.astype(jnp.float32).reshape(sequences, block_count, block_len, head_count, array.shape[-1])
        return jnp.swapaxes(shaped, 0, 1)
    log_decay = -rates.astype(jnp.float32)
    offsets = jnp.arange(block_len, dtype=jnp.float32)
    decay_query = jnp.exp(log_decay[None, :] * (offsets[:, None] + 1.0))
    distance = offsets[:, None] - offsets[None, :]
    decay_mask = jnp.where(distance[None] >= 0.0, jnp.exp(log_decay[:, None, None] * jnp.maximum(distance, 0.0)[None]), 0.0)
    decay_key = jnp.exp(log_decay[None, :] * (block_len - 1.0 - offsets[:, None]))
    decay_block = jnp.exp(log_decay * block_len)
    highest = lax.Precision.HIGHEST

    def advance(memory_state, pieces):
        query_block, key_block, value_block = pieces
        carried = jnp.einsum('slhk,shkv->slhv', query_block, memory_state, precision=highest) * decay_query[None, :, :, None]
        scores = jnp.einsum('slhk,smhk->shlm', query_block, key_block, precision=highest) * decay_mask[None]
        within = jnp.einsum('shlm,smhv->slhv', scores, value_block, precision=highest)
        weighted = key_block * decay_key[None, :, :, None]
        memory_state = decay_block[None, :, None, None] * memory_state + jnp.einsum('slhk,slhv->shkv', weighted, value_block, precision=highest)
        return (memory_state, carried + within)
    initial = jnp.zeros((sequences, head_count, key_dim, value_dim), jnp.float32)
    _, outputs = lax.scan(advance, initial, (blocked(ret_query), blocked(ret_key), blocked(ret_value)))
    return jnp.swapaxes(outputs, 0, 1).reshape(tokens_all, head_count, value_dim)

def reference(tokens, w_query, w_key, w_value, w_mem_query, w_mem_key, w_mem_value, w_gate, w_lift, decay_rate, store, passage_ids):
    total_rows = tokens.shape[0]
    head_count = decay_rate.shape[0]
    highest = lax.Precision.HIGHEST
    features = tokens.astype(jnp.float32)
    row_scale = lax.rsqrt(lax.optimization_barrier(jnp.mean(features * features, axis=1, keepdims=True)) + norm_eps)
    positions = jnp.arange(total_rows, dtype=jnp.int32) % SEQ_LEN

    def project(weight):
        return jnp.dot(tokens, weight, preferred_element_type=jnp.float32)
    ret_query = rotate((project(w_query) * row_scale).reshape(total_rows, head_count, KEY_DIM), positions).astype(jnp.bfloat16)
    ret_key = (rotate((project(w_key) * row_scale).reshape(total_rows, head_count, KEY_DIM), positions) * KEY_DIM ** (-0.5)).astype(jnp.bfloat16)
    ret_value = (project(w_value) * row_scale).astype(jnp.bfloat16).reshape(total_rows, head_count, VALUE_DIM)
    mem_query = head_norm(project(w_mem_query).reshape(total_rows, head_count, MEM_DIM)).astype(jnp.bfloat16)
    gate_value = jax.nn.sigmoid(project(w_gate) * row_scale)
    ret_norm = group_norm(retention(ret_query, ret_key, ret_value, decay_rate, RET_BLOCK))

    def passage_rows(ident):
        passage = lax.dynamic_index_in_dim(store, ident, 0, keepdims=False)
        key_part = head_norm(jnp.dot(passage, w_mem_key, preferred_element_type=jnp.float32).reshape(PASS_ROWS, head_count, MEM_DIM))
        value_part = jnp.dot(passage, w_mem_value, preferred_element_type=jnp.float32).reshape(PASS_ROWS, head_count, MEM_DIM)
        return (key_part.astype(jnp.bfloat16), value_part.astype(jnp.bfloat16))
    pass_key, pass_value = lax.map(passage_rows, passage_ids.reshape(-1).astype(jnp.int32))
    block_count, picks = passage_ids.shape
    query_blocks = mem_query.reshape(block_count, BLOCK, head_count, MEM_DIM)
    key_blocks = pass_key.reshape(block_count, picks, PASS_ROWS, head_count, MEM_DIM)
    value_blocks = pass_value.reshape(block_count, picks, PASS_ROWS, head_count, MEM_DIM)

    def attend(pieces):
        query_block, key_block, value_block = pieces
        scores = jnp.einsum('thd,prhd->hptr', query_block.astype(jnp.float32), key_block.astype(jnp.float32), precision=highest) * MEM_DIM ** (-0.5)
        exponent = jnp.exp(scores)
        mass_sum = lax.optimization_barrier(jnp.sum(exponent, axis=3))
        rounded = lax.optimization_barrier(exponent.astype(jnp.bfloat16)).astype(jnp.float32)
        partial_value = jnp.einsum('hptr,prhd->pthd', rounded, value_block.astype(jnp.float32), precision=highest)
        partial_value = lax.optimization_barrier(partial_value.astype(jnp.bfloat16)).astype(jnp.float32)
        summed = lax.optimization_barrier(jnp.sum(partial_value, axis=0))
        return summed / jnp.swapaxes(lax.optimization_barrier(jnp.sum(mass_sum, axis=1)), 0, 1)[:, :, None]
    mem_out = lax.map(attend, (query_blocks, key_blocks, value_blocks)).reshape(total_rows, head_count, MEM_DIM).astype(jnp.bfloat16)
    mem_lift = jnp.einsum('thd,hde->the', mem_out.astype(jnp.float32), w_lift.astype(jnp.float32), precision=highest)
    mixed = (ret_norm + gate_value[:, :, None] * mem_lift).astype(jnp.bfloat16)
    return mixed.reshape(total_rows, head_count * VALUE_DIM)
```

```python
import jax
import jax.numpy as jnp
import numpy as np
from jax import lax
from jax.experimental import pallas as pl
from jax.experimental.pallas import tpu as pltpu
from jax.sharding import PartitionSpec as P

D = 4096
KEY_DIM = 128
VALUE_DIM = 256
MEM_DIM = 128
SEQ_LEN = 512
BLOCK = 128
PICKS = 2
PASS_ROWS = 64
PASS_SHIFT = 7
N_ST = 16
RING = 8
BLOCKS = 4
SLOTS = 14
HALF = 256
TOK_COLS = 640

norm_eps = 1e-06
rope_base = 10000.0

F32 = jnp.float32
BF16 = jnp.bfloat16
MESH = pl.DeviceIdType.MESH


def rotary_tables():
    half = KEY_DIM // 2
    inverse = rope_base ** (-np.arange(half, dtype=np.float64) / half)
    angles = np.arange(SEQ_LEN, dtype=np.float64)[:, None] * inverse[None, :]
    cosine, sine = np.cos(angles), np.sin(angles)
    cos_table = np.concatenate([cosine, cosine], axis=1).astype(np.float32)
    sin_table = np.concatenate([-sine, sine], axis=1).astype(np.float32)
    return cos_table, sin_table


def dot(a, b):
    return jnp.dot(a, b, preferred_element_type=F32)


def dot_t(a, b):
    return lax.dot_general(a, b, (((1,), (1,)), ((), ())), preferred_element_type=F32)


def kernel(
    tok,
    wq,
    wk,
    wv,
    wmq,
    wmk,
    wmv,
    wg,
    wl,
    store,
    cos_in,
    sin_in,
    decay,
    ids,
    out,
    x,
    wt,
    wm,
    store_v,
    outbox,
    inbox,
    acc,
    squares,
    gates,
    acc_p,
    key_v,
    value_v,
    mem_q,
    gate_v,
    ret_norm,
    wg_v,
    wg_f,
    wl_v,
    cos_v,
    sin_v,
    out_v,
    ids_all,
    tok_sem,
    local_sem,
    out_sem,
    z_send,
    z_recv,
    d_send,
    d_recv,
    i_send,
    i_recv,
    s_send,
    s_recv,
):
    st = lax.axis_index("st")
    tp = lax.axis_index("tp")
    z = lax.div(tp, 2)
    core = lax.rem(tp, 2)
    other = 1 - core
    up = lax.rem(z + 1, RING) * 2 + core
    down = lax.rem(z + RING - 1, RING) * 2 + core
    partner = z * 2 + other

    def peer(offset):
        return lax.rem(st + offset, N_ST)

    tok_copies = [
        pltpu.make_async_copy(
            tok.at[pl.ds(b * BLOCK, BLOCK), :], x.at[0, z, b, core], tok_sem.at[b]
        )
        for b in range(BLOCKS)
    ]
    for copy in tok_copies:
        copy.start()
    local = [
        (wg, wg_v),
        (wq, wt.at[:, pl.ds(0, 128)]),
        (wk, wt.at[:, pl.ds(128, 128)]),
        (wv, wt.at[:, pl.ds(256, 256)]),
        (wmq, wt.at[:, pl.ds(512, 128)]),
        (store, store_v),
        (wmk, wm.at[:, pl.ds(0, 128)]),
        (wmv, wm.at[:, pl.ds(128, 128)]),
        (wl, wl_v),
        (cos_in, cos_v),
        (sin_in, sin_v),
    ]
    local_copies = [
        pltpu.make_async_copy(src, dst, local_sem.at[i]) for i, (src, dst) in enumerate(local)
    ]
    for copy in local_copies:
        copy.start()

    barrier = pltpu.get_barrier_semaphore()
    for target in (up, down, partner):
        pl.semaphore_signal(barrier, inc=1, device_id={"tp": target}, device_id_type=MESH)

    @pl.loop(1, N_ST)
    def _(offset):
        pl.semaphore_signal(
            barrier, inc=1, device_id={"st": peer(offset)}, device_id_type=MESH
        )

    pl.semaphore_wait(barrier, 3 + N_ST - 1)

    def slot_block(d, s):
        return lax.rem(s + 2 * d, BLOCKS)

    def chunk_at(d, hops):
        return lax.rem(z + RING - hops, RING) if d == 0 else lax.rem(z + hops, RING)

    def z_copy(phase, d, s):
        ref = x.at[phase, chunk_at(d, lax.div(s, BLOCKS)), slot_block(d, s), core]
        return pltpu.make_async_remote_copy(
            src_ref=ref,
            dst_ref=ref,
            send_sem=z_send.at[phase, d, s],
            recv_sem=z_recv.at[phase, d, s],
            device_id={"tp": up if d == 0 else down},
            device_id_type=MESH,
        )

    def z_arrival(phase, d, s):
        ref = x.at[phase, chunk_at(d, lax.div(s, BLOCKS) + 1), slot_block(d, s), core]
        return pltpu.make_async_remote_copy(
            src_ref=ref,
            dst_ref=ref,
            send_sem=z_send.at[phase, d, s],
            recv_sem=z_recv.at[phase, d, s],
            device_id={"tp": up if d == 0 else down},
            device_id_type=MESH,
        )

    def d_copy(phase, index, chunk, b, half):
        ref = x.at[phase, chunk, b, half]
        return pltpu.make_async_remote_copy(
            src_ref=ref,
            dst_ref=ref,
            send_sem=d_send.at[phase, index],
            recv_sem=d_recv.at[phase, index],
            device_id={"tp": partner},
            device_id_type=MESH,
        )

    def d_slot(d, s):
        return BLOCKS + d * SLOTS + s

    def send_own(phase):
        for b in range(BLOCKS):
            z_copy(phase, 0, jnp.int32(b)).start()
            z_copy(phase, 1, jnp.int32(b)).start()
        for b in range(BLOCKS):
            d_copy(phase, b, z, b, core).start()

    for copy in tok_copies:
        copy.wait()
    send_own(0)

    def id_copy(offset):
        return pltpu.make_async_remote_copy(
            src_ref=ids,
            dst_ref=ids_all.at[st],
            send_sem=i_send.at[offset],
            recv_sem=i_recv.at[offset],
            device_id={"st": peer(offset)},
            device_id_type=MESH,
        )

    @pl.loop(1, N_ST)
    def _(offset):
        id_copy(offset).start()

    local_copies[0].wait()
    for chunk in range(RING):
        wg_f[chunk] = wg_v[:, chunk * 512 : (chunk + 1) * 512].astype(F32)
    for copy in local_copies[1:]:
        copy.wait()

    def add_tokens(chunk, b, first=False):
        both = jnp.concatenate([x[0, chunk, b, 0], x[0, chunk, b, 1]], axis=1)
        rows = pl.ds(pl.multiple_of(chunk * 512, 512), 512)
        product = dot(both, wt[rows, :])
        wide = both.astype(F32)
        square = wide * wide
        gated = wide * wg_f[chunk]
        square = (square[:, 0:128] + square[:, 128:256]) + (
            square[:, 256:384] + square[:, 384:512]
        )
        gated = (gated[:, 0:128] + gated[:, 128:256]) + (gated[:, 256:384] + gated[:, 384:512])
        if first:
            acc[b] = product
            squares[b] = square
            gates[b] = gated
        else:
            acc[b] += product
            squares[b] += square
            gates[b] += gated

    def add_passages(chunk, b, first=False):
        both = jnp.concatenate([x[1, chunk, b, 0], x[1, chunk, b, 1]], axis=1)
        rows = pl.ds(pl.multiple_of(chunk * 512, 512), 512)
        product = dot(both, wm[rows, :])
        if first:
            acc_p[b] = product
        else:
            acc_p[b] += product

    def take_slot(phase, s, relay):
        for d in range(2):
            z_arrival(phase, d, s).wait_recv()
            if relay is True:
                z_copy(phase, d, s + BLOCKS).start()
            elif relay is not False:

                @pl.when(relay)
                def _():
                    z_copy(phase, d, s + BLOCKS).start()

            chunk = chunk_at(d, lax.div(s, BLOCKS) + 1)
            d_copy(phase, d_slot(d, s), chunk, slot_block(d, s), core).start()

    def add_slot(phase, s):
        for d in range(2):
            chunk = chunk_at(d, lax.div(s, BLOCKS) + 1)
            b = slot_block(d, s)
            d_copy(phase, d_slot(d, s), chunk, b, other).wait_recv()
            if phase == 0:
                add_tokens(chunk, b)
            else:
                add_passages(chunk, b)

    for b in range(BLOCKS):
        d_copy(0, b, z, b, other).wait_recv()
        add_tokens(z, b, first=True)

    def id_arrival(offset):
        return pltpu.make_async_remote_copy(
            src_ref=ids,
            dst_ref=ids_all.at[peer(N_ST - offset)],
            send_sem=i_send.at[offset],
            recv_sem=i_recv.at[offset],
            device_id={"st": peer(offset)},
            device_id_type=MESH,
        )

    take_slot(0, jnp.int32(0), True)

    @pl.loop(1, N_ST)
    def _(offset):
        id_arrival(offset).wait_recv()

    def wanted_row(read):
        row = jnp.int32(0)
        for pick in range(PICKS):
            for b in range(BLOCKS):
                ident = read(pick, b)
                mine = lax.shift_right_logical(ident, PASS_SHIFT) == st
                row = row + jnp.where(mine, ident & ((1 << PASS_SHIFT) - 1), 0)
        return row

    inbox[st] = store_v[wanted_row(lambda pick, b: ids[pick, b])]

    @pl.loop(1, N_ST)
    def _(offset):
        target = peer(offset)
        outbox[offset] = store_v[wanted_row(lambda pick, b: ids_all[target, pick, b])]

    take_slot(0, jnp.int32(1), True)
    add_slot(0, jnp.int32(0))

    def row_copy(offset, place):
        return pltpu.make_async_remote_copy(
            src_ref=outbox.at[offset],
            dst_ref=inbox.at[place],
            send_sem=s_send.at[offset],
            recv_sem=s_recv.at[offset],
            device_id={"st": peer(offset)},
            device_id_type=MESH,
        )

    @pl.loop(1, N_ST)
    def _(offset):
        row_copy(offset, st).start()

    @pl.loop(2, 9)
    def _(s):
        take_slot(0, s, True)
        add_slot(0, s - 1)

    @pl.loop(1, N_ST)
    def _(offset):
        row_copy(offset, peer(N_ST - offset)).wait_recv()

    for b in range(BLOCKS):
        for pick in range(PICKS):
            owner = lax.shift_right_logical(ids[pick, b], PASS_SHIFT)
            x[1, z, b, core, pick * PASS_ROWS : (pick + 1) * PASS_ROWS, :] = inbox[owner]

    take_slot(0, jnp.int32(9), True)
    add_slot(0, jnp.int32(8))
    send_own(1)

    @pl.loop(10, SLOTS)
    def _(s):
        take_slot(0, s, False)
        add_slot(0, s - 1)

    rate = decay[0]

    def finish_tokens(b):
        mean_square = jnp.sum(squares[b], axis=1, keepdims=True) * (1.0 / D)
        scale = lax.rsqrt(mean_square + norm_eps)
        cosine = cos_v[b * BLOCK : (b + 1) * BLOCK, :]
        sine = sin_v[b * BLOCK : (b + 1) * BLOCK, :]

        def rotate(values):
            return values * cosine + pltpu.roll(values, KEY_DIM // 2, 1) * sine

        query = rotate(acc[b, :, 0:128] * scale).astype(BF16)
        key = (rotate(acc[b, :, 128:256] * scale) * KEY_DIM ** (-0.5)).astype(BF16)
        key_v[b * BLOCK : (b + 1) * BLOCK, :] = key
        value_v[b * BLOCK : (b + 1) * BLOCK, :] = (acc[b, :, 256:512] * scale).astype(BF16)
        memory = acc[b, :, 512:640]
        mean = jnp.mean(memory * memory, axis=1, keepdims=True)
        mem_q[b] = (memory * lax.rsqrt(mean + norm_eps)).astype(BF16)
        gate = jnp.sum(gates[b], axis=1, keepdims=True) * scale
        gate_v[b] = jnp.broadcast_to(jax.nn.sigmoid(gate), (BLOCK, 128))

        span = (b + 1) * BLOCK
        keys = key_v[0:span, :]
        values = value_v[0:span, :]
        row = lax.broadcasted_iota(jnp.int32, (BLOCK, span), 0) + b * BLOCK
        column = lax.broadcasted_iota(jnp.int32, (BLOCK, span), 1)
        distance = (row - column).astype(F32)
        mask = jnp.where(distance >= 0.0, jnp.exp(-rate * jnp.maximum(distance, 0.0)), 0.0)
        scores = dot_t(query, keys) * mask
        upper = scores.astype(BF16)
        lower = (scores - upper.astype(F32)).astype(BF16)
        mixed = dot(upper, values) + dot(lower, values)
        centred = mixed - jnp.mean(mixed, axis=1, keepdims=True)
        variance = jnp.mean(centred * centred, axis=1, keepdims=True)
        ret_norm[b] = centred * lax.rsqrt(variance + norm_eps)

    def out_copy(b):
        return pltpu.make_async_copy(
            out_v.at[b], out.at[pl.ds(b * BLOCK, BLOCK), :], out_sem.at[b]
        )

    def finish_block(b):
        raw = acc_p[b, :, 0:128]
        mean = jnp.mean(raw * raw, axis=1, keepdims=True)
        pass_key = (raw * lax.rsqrt(mean + norm_eps)).astype(BF16)
        pass_value = acc_p[b, :, 128:256].astype(BF16)
        exponent = jnp.exp(dot_t(mem_q[b], pass_key) * MEM_DIM ** (-0.5))
        mass = jnp.sum(exponent, axis=1, keepdims=True)
        summed = dot(exponent.astype(BF16), pass_value)
        mem_out = (summed / mass).astype(BF16)
        lift = dot(mem_out, wl_v[0])
        gate = gate_v[b]
        gate = jnp.concatenate([gate, gate], axis=1)
        out_v[b] = (ret_norm[b] + gate * lift).astype(BF16)
        out_copy(b).start()

    for s in range(SLOTS):
        take_slot(1, jnp.int32(s), s < SLOTS - BLOCKS)
        if s == 0:
            add_slot(0, jnp.int32(SLOTS - 1))
            for b in range(BLOCKS):
                d_copy(1, b, z, b, other).wait_recv()
                add_passages(z, b, first=True)
        else:
            add_slot(1, jnp.int32(s - 1))
        if s < BLOCKS:
            finish_tokens(s)
        if s == 8:

            @pl.loop(0, SLOTS)
            def _(n):
                z_copy(0, 0, n).wait_send()
                z_copy(0, 1, n).wait_send()

            @pl.loop(0, BLOCKS + 2 * SLOTS)
            def _(n):
                d_copy(0, n, z, 0, core).wait_send()

            @pl.loop(1, N_ST)
            def _(offset):
                id_copy(offset).wait_send()
                row_copy(offset, st).wait_send()

    finish_block(0)
    finish_block(2)
    add_slot(1, jnp.int32(SLOTS - 1))
    finish_block(1)
    finish_block(3)

    @pl.loop(0, SLOTS)
    def _(n):
        z_copy(1, 0, n).wait_send()
        z_copy(1, 1, n).wait_send()

    @pl.loop(0, BLOCKS + 2 * SLOTS)
    def _(n):
        d_copy(1, n, z, 0, core).wait_send()

    for b in range(BLOCKS):
        out_copy(b).wait()


def per_device(
    tokens,
    w_query,
    w_key,
    w_value,
    w_mem_query,
    w_mem_key,
    w_mem_value,
    w_gate,
    w_lift,
    decay_rate,
    store,
    passage_ids,
):
    cos_table, sin_table = rotary_tables()
    hbm = pl.BlockSpec(memory_space=pl.ANY)
    smem = pl.BlockSpec(memory_space=pltpu.SMEM)
    dma = pltpu.SemaphoreType.DMA
    return pl.pallas_call(
        kernel,
        out_shape=jax.ShapeDtypeStruct((SEQ_LEN, VALUE_DIM), BF16),
        in_specs=[hbm] * 12 + [smem] * 2,
        out_specs=hbm,
        scratch_shapes=[
            pltpu.VMEM((2, RING, BLOCKS, 2, BLOCK, HALF), BF16),
            pltpu.VMEM((D, TOK_COLS), BF16),
            pltpu.VMEM((D, 2 * MEM_DIM), BF16),
            pltpu.VMEM(store.shape, BF16),
            pltpu.VMEM((N_ST, PASS_ROWS, HALF), BF16),
            pltpu.VMEM((N_ST, PASS_ROWS, HALF), BF16),
            pltpu.VMEM((BLOCKS, BLOCK, TOK_COLS), F32),
            pltpu.VMEM((BLOCKS, BLOCK, 128), F32),
            pltpu.VMEM((BLOCKS, BLOCK, 128), F32),
            pltpu.VMEM((BLOCKS, BLOCK, 2 * MEM_DIM), F32),
            pltpu.VMEM((SEQ_LEN, KEY_DIM), BF16),
            pltpu.VMEM((SEQ_LEN, VALUE_DIM), BF16),
            pltpu.VMEM((BLOCKS, BLOCK, MEM_DIM), BF16),
            pltpu.VMEM((BLOCKS, BLOCK, 128), F32),
            pltpu.VMEM((BLOCKS, BLOCK, VALUE_DIM), F32),
            pltpu.VMEM((1, D), BF16),
            pltpu.VMEM((RING, 1, 512), F32),
            pltpu.VMEM((1, MEM_DIM, VALUE_DIM), BF16),
            pltpu.VMEM((SEQ_LEN, KEY_DIM), F32),
            pltpu.VMEM((SEQ_LEN, KEY_DIM), F32),
            pltpu.VMEM((BLOCKS, BLOCK, VALUE_DIM), BF16),
            pltpu.SMEM((N_ST, PICKS, BLOCKS), jnp.int32),
            dma((BLOCKS,)),
            dma((11,)),
            dma((BLOCKS,)),
            dma((2, 2, SLOTS)),
            dma((2, 2, SLOTS)),
            dma((2, BLOCKS + 2 * SLOTS)),
            dma((2, BLOCKS + 2 * SLOTS)),
            dma((N_ST,)),
            dma((N_ST,)),
            dma((N_ST,)),
            dma((N_ST,)),
        ],
        compiler_params=pltpu.CompilerParams(
            collective_id=0, has_side_effects=True, vmem_limit_bytes=48 * 1024 * 1024
        ),
        name="fused_layer",
    )(
        tokens,
        w_query,
        w_key,
        w_value,
        w_mem_query,
        w_mem_key,
        w_mem_value,
        w_gate.reshape(1, D),
        w_lift,
        store,
        cos_table,
        sin_table,
        decay_rate,
        passage_ids.T,
    )


def solution(mesh):
    in_specs = (
        P("st", "tp"),
        P(None, "tp"),
        P(None, "tp"),
        P(None, "tp"),
        P(None, "tp"),
        P(None, "tp"),
        P(None, "tp"),
        P(None, "tp"),
        P("tp", None, None),
        P("tp"),
        P("st", None, "tp"),
        P("st", None),
    )
    out_specs = P("st", "tp")
    return jax.shard_map(
        per_device, mesh=mesh, in_specs=in_specs, out_specs=out_specs, check_vma=False
    )
```

```python
import jax
import jax.numpy as jnp
import numpy as np
from jax import lax
from jax.experimental import pallas as pl
from jax.experimental.pallas import tpu as pltpu
from jax.sharding import PartitionSpec as P

D = 4096
KEY_DIM = 128
VALUE_DIM = 256
MEM_DIM = 128
SEQ_LEN = 512
BLOCK = 128
PICKS = 2
PASS_ROWS = 64
PASS_SHIFT = 7
N_ST = 16
RING = 8
BLOCKS = 4
SLOTS = 14
HALF = 256
TOK_COLS = 640

norm_eps = 1e-06
rope_base = 10000.0

F32 = jnp.float32
BF16 = jnp.bfloat16
MESH = pl.DeviceIdType.MESH


def rotary_tables():
    half = KEY_DIM // 2
    inverse = rope_base ** (-np.arange(half, dtype=np.float64) / half)
    angles = np.arange(SEQ_LEN, dtype=np.float64)[:, None] * inverse[None, :]
    cosine, sine = np.cos(angles), np.sin(angles)
    cos_table = np.concatenate([cosine, cosine], axis=1).astype(np.float32)
    sin_table = np.concatenate([-sine, sine], axis=1).astype(np.float32)
    return cos_table, sin_table


def dot(a, b):
    return jnp.dot(a, b, preferred_element_type=F32)


def dot_t(a, b):
    return lax.dot_general(a, b, (((1,), (1,)), ((), ())), preferred_element_type=F32)


def kernel(
    tok,
    wq,
    wk,
    wv,
    wmq,
    wmk,
    wmv,
    wg,
    wl,
    store,
    cos_in,
    sin_in,
    decay,
    ids,
    out,
    x,
    wt,
    wm,
    store_v,
    outbox,
    inbox,
    acc,
    squares,
    gates,
    acc_p,
    key_v,
    value_v,
    mem_q,
    gate_v,
    ret_norm,
    wg_v,
    wg_f,
    wl_v,
    cos_v,
    sin_v,
    out_v,
    ids_all,
    tok_sem,
    local_sem,
    out_sem,
    z_send,
    z_recv,
    d_send,
    d_recv,
    i_send,
    i_recv,
    s_send,
    s_recv,
):
    st = lax.axis_index("st")
    tp = lax.axis_index("tp")
    z = lax.div(tp, 2)
    core = lax.rem(tp, 2)
    other = 1 - core
    up = lax.rem(z + 1, RING) * 2 + core
    down = lax.rem(z + RING - 1, RING) * 2 + core
    partner = z * 2 + other

    def peer(offset):
        return lax.rem(st + offset, N_ST)

    tok_copies = [
        pltpu.make_async_copy(
            tok.at[pl.ds(b * BLOCK, BLOCK), :], x.at[0, z, b, core], tok_sem.at[b]
        )
        for b in range(BLOCKS)
    ]
    for copy in tok_copies:
        copy.start()
    local = [
        (wg, wg_v),
        (wq, wt.at[:, pl.ds(0, 128)]),
        (wk, wt.at[:, pl.ds(128, 128)]),
        (wv, wt.at[:, pl.ds(256, 256)]),
        (wmq, wt.at[:, pl.ds(512, 128)]),
        (store, store_v),
        (wmk, wm.at[:, pl.ds(0, 128)]),
        (wmv, wm.at[:, pl.ds(128, 128)]),
        (wl, wl_v),
        (cos_in, cos_v),
        (sin_in, sin_v),
    ]
    local_copies = [
        pltpu.make_async_copy(src, dst, local_sem.at[i]) for i, (src, dst) in enumerate(local)
    ]
    for copy in local_copies:
        copy.start()

    barrier = pltpu.get_barrier_semaphore()
    for target in (up, down, partner):
        pl.semaphore_signal(barrier, inc=1, device_id={"tp": target}, device_id_type=MESH)

    @pl.loop(1, N_ST)
    def _(offset):
        pl.semaphore_signal(
            barrier, inc=1, device_id={"st": peer(offset)}, device_id_type=MESH
        )

    pl.semaphore_wait(barrier, 3 + N_ST - 1)

    def slot_block(d, s):
        return lax.rem(s + 2 * d, BLOCKS)

    def chunk_at(d, hops):
        return lax.rem(z + RING - hops, RING) if d == 0 else lax.rem(z + hops, RING)

    def z_copy(phase, d, s):
        ref = x.at[phase, chunk_at(d, lax.div(s, BLOCKS)), slot_block(d, s), core]
        return pltpu.make_async_remote_copy(
            src_ref=ref,
            dst_ref=ref,
            send_sem=z_send.at[phase, d, s],
            recv_sem=z_recv.at[phase, d, s],
            device_id={"tp": up if d == 0 else down},
            device_id_type=MESH,
        )

    def z_arrival(phase, d, s):
        ref = x.at[phase, chunk_at(d, lax.div(s, BLOCKS) + 1), slot_block(d, s), core]
        return pltpu.make_async_remote_copy(
            src_ref=ref,
            dst_ref=ref,
            send_sem=z_send.at[phase, d, s],
            recv_sem=z_recv.at[phase, d, s],
            device_id={"tp": up if d == 0 else down},
            device_id_type=MESH,
        )

    def d_copy(phase, index, chunk, b, half):
        ref = x.at[phase, chunk, b, half]
        return pltpu.make_async_remote_copy(
            src_ref=ref,
            dst_ref=ref,
            send_sem=d_send.at[phase, index],
            recv_sem=d_recv.at[phase, index],
            device_id={"tp": partner},
            device_id_type=MESH,
        )

    def d_slot(d, s):
        return BLOCKS + d * SLOTS + s

    def send_own(phase):
        for b in range(BLOCKS):
            z_copy(phase, 0, jnp.int32(b)).start()
            z_copy(phase, 1, jnp.int32(b)).start()
        for b in range(BLOCKS):
            d_copy(phase, b, z, b, core).start()

    for copy in tok_copies:
        copy.wait()
    send_own(0)

    def id_copy(offset):
        return pltpu.make_async_remote_copy(
            src_ref=ids,
            dst_ref=ids_all.at[st],
            send_sem=i_send.at[offset],
            recv_sem=i_recv.at[offset],
            device_id={"st": peer(offset)},
            device_id_type=MESH,
        )

    @pl.loop(1, N_ST)
    def _(offset):
        id_copy(offset).start()

    local_copies[0].wait()
    for chunk in range(RING):
        wg_f[chunk] = wg_v[:, chunk * 512 : (chunk + 1) * 512].astype(F32)
    for copy in local_copies[1:]:
        copy.wait()

    def add_tokens(chunk, b, first=False):
        both = jnp.concatenate([x[0, chunk, b, 0], x[0, chunk, b, 1]], axis=1)
        rows = pl.ds(pl.multiple_of(chunk * 512, 512), 512)
        product = dot(both, wt[rows, :])
        wide = both.astype(F32)
        square = wide * wide
        gated = wide * wg_f[chunk]
        square = (square[:, 0:128] + square[:, 128:256]) + (
            square[:, 256:384] + square[:, 384:512]
        )
        gated = (gated[:, 0:128] + gated[:, 128:256]) + (gated[:, 256:384] + gated[:, 384:512])
        if first:
            acc[b] = product
            squares[b] = square
            gates[b] = gated
        else:
            acc[b] += product
            squares[b] += square
            gates[b] += gated

    def add_passages(chunk, b, first=False):
        both = jnp.concatenate([x[1, chunk, b, 0], x[1, chunk, b, 1]], axis=1)
        rows = pl.ds(pl.multiple_of(chunk * 512, 512), 512)
        product = dot(both, wm[rows, :])
        if first:
            acc_p[b] = product
        else:
            acc_p[b] += product

    def take_slot(phase, s, relay):
        for d in range(2):
            z_arrival(phase, d, s).wait_recv()
            if relay is True:
                z_copy(phase, d, s + BLOCKS).start()
            elif relay is not False:

                @pl.when(relay)
                def _():
                    z_copy(phase, d, s + BLOCKS).start()

            chunk = chunk_at(d, lax.div(s, BLOCKS) + 1)
            d_copy(phase, d_slot(d, s), chunk, slot_block(d, s), core).start()

    def add_slot(phase, s):
        for d in range(2):
            chunk = chunk_at(d, lax.div(s, BLOCKS) + 1)
            b = slot_block(d, s)
            d_copy(phase, d_slot(d, s), chunk, b, other).wait_recv()
            if phase == 0:
                add_tokens(chunk, b)
            else:
                add_passages(chunk, b)

    for b in range(BLOCKS):
        d_copy(0, b, z, b, other).wait_recv()
        add_tokens(z, b, first=True)

    def id_arrival(offset):
        return pltpu.make_async_remote_copy(
            src_ref=ids,
            dst_ref=ids_all.at[peer(N_ST - offset)],
            send_sem=i_send.at[offset],
            recv_sem=i_recv.at[offset],
            device_id={"st": peer(offset)},
            device_id_type=MESH,
        )

    take_slot(0, jnp.int32(0), True)

    @pl.loop(1, N_ST)
    def _(offset):
        id_arrival(offset).wait_recv()

    def wanted_row(read):
        row = jnp.int32(0)
        for pick in range(PICKS):
            for b in range(BLOCKS):
                ident = read(pick, b)
                mine = lax.shift_right_logical(ident, PASS_SHIFT) == st
                row = row + jnp.where(mine, ident & ((1 << PASS_SHIFT) - 1), 0)
        return row

    inbox[st] = store_v[wanted_row(lambda pick, b: ids[pick, b])]

    @pl.loop(1, N_ST)
    def _(offset):
        target = peer(offset)
        outbox[offset] = store_v[wanted_row(lambda pick, b: ids_all[target, pick, b])]

    take_slot(0, jnp.int32(1), True)
    add_slot(0, jnp.int32(0))

    def row_copy(offset, place):
        return pltpu.make_async_remote_copy(
            src_ref=outbox.at[offset],
            dst_ref=inbox.at[place],
            send_sem=s_send.at[offset],
            recv_sem=s_recv.at[offset],
            device_id={"st": peer(offset)},
            device_id_type=MESH,
        )

    @pl.loop(1, N_ST)
    def _(offset):
        row_copy(offset, st).start()

    @pl.loop(2, 9)
    def _(s):
        take_slot(0, s, True)
        add_slot(0, s - 1)

    @pl.loop(1, N_ST)
    def _(offset):
        row_copy(offset, peer(N_ST - offset)).wait_recv()

    for b in range(BLOCKS):
        for pick in range(PICKS):
            owner = lax.shift_right_logical(ids[pick, b], PASS_SHIFT)
            x[1, z, b, core, pick * PASS_ROWS : (pick + 1) * PASS_ROWS, :] = inbox[owner]

    take_slot(0, jnp.int32(9), True)
    add_slot(0, jnp.int32(8))
    send_own(1)

    @pl.loop(10, SLOTS)
    def _(s):
        take_slot(0, s, False)
        add_slot(0, s - 1)

    rate = decay[0]

    def finish_tokens(b):
        mean_square = jnp.sum(squares[b], axis=1, keepdims=True) * (1.0 / D)
        scale = lax.rsqrt(mean_square + norm_eps)
        cosine = cos_v[b * BLOCK : (b + 1) * BLOCK, :]
        sine = sin_v[b * BLOCK : (b + 1) * BLOCK, :]

        def rotate(values):
            return values * cosine + pltpu.roll(values, KEY_DIM // 2, 1) * sine

        query = rotate(acc[b, :, 0:128] * scale).astype(BF16)
        key = (rotate(acc[b, :, 128:256] * scale) * KEY_DIM ** (-0.5)).astype(BF16)
        key_v[b * BLOCK : (b + 1) * BLOCK, :] = key
        value_v[b * BLOCK : (b + 1) * BLOCK, :] = (acc[b, :, 256:512] * scale).astype(BF16)
        memory = acc[b, :, 512:640]
        mean = jnp.mean(memory * memory, axis=1, keepdims=True)
        mem_q[b] = (memory * lax.rsqrt(mean + norm_eps)).astype(BF16)
        gate = jnp.sum(gates[b], axis=1, keepdims=True) * scale
        gate_v[b] = jnp.broadcast_to(jax.nn.sigmoid(gate), (BLOCK, 128))

        span = (b + 1) * BLOCK
        keys = key_v[0:span, :]
        values = value_v[0:span, :]
        row = lax.broadcasted_iota(jnp.int32, (BLOCK, span), 0) + b * BLOCK
        column = lax.broadcasted_iota(jnp.int32, (BLOCK, span), 1)
        distance = (row - column).astype(F32)
        mask = jnp.where(distance >= 0.0, jnp.exp(-rate * jnp.maximum(distance, 0.0)), 0.0)
        scores = dot_t(query, keys) * mask
        upper = scores.astype(BF16)
        lower = (scores - upper.astype(F32)).astype(BF16)
        mixed = dot(upper, values) + dot(lower, values)
        centred = mixed - jnp.mean(mixed, axis=1, keepdims=True)
        variance = jnp.mean(centred * centred, axis=1, keepdims=True)
        ret_norm[b] = centred * lax.rsqrt(variance + norm_eps)

    def out_copy(b):
        return pltpu.make_async_copy(
            out_v.at[b], out.at[pl.ds(b * BLOCK, BLOCK), :], out_sem.at[b]
        )

    def finish_block(b):
        raw = acc_p[b, :, 0:128]
        mean = jnp.mean(raw * raw, axis=1, keepdims=True)
        pass_key = (raw * lax.rsqrt(mean + norm_eps)).astype(BF16)
        pass_value = acc_p[b, :, 128:256].astype(BF16)
        exponent = jnp.exp(dot_t(mem_q[b], pass_key) * MEM_DIM ** (-0.5))
        mass = jnp.sum(exponent, axis=1, keepdims=True)
        summed = dot(exponent.astype(BF16), pass_value)
        mem_out = (summed / mass).astype(BF16)
        lift = dot(mem_out, wl_v[0])
        gate = gate_v[b]
        gate = jnp.concatenate([gate, gate], axis=1)
        out_v[b] = (ret_norm[b] + gate * lift).astype(BF16)
        out_copy(b).start()

    for s in range(SLOTS):
        take_slot(1, jnp.int32(s), s < SLOTS - BLOCKS)
        if s == 0:
            add_slot(0, jnp.int32(SLOTS - 1))
            for b in range(BLOCKS):
                d_copy(1, b, z, b, other).wait_recv()
                add_passages(z, b, first=True)
        else:
            add_slot(1, jnp.int32(s - 1))
        if s < BLOCKS:
            finish_tokens(s)
        if s == 8:

            @pl.loop(0, SLOTS)
            def _(n):
                z_copy(0, 0, n).wait_send()
                z_copy(0, 1, n).wait_send()

            @pl.loop(0, BLOCKS + 2 * SLOTS)
            def _(n):
                d_copy(0, n, z, 0, core).wait_send()

            @pl.loop(1, N_ST)
            def _(offset):
                id_copy(offset).wait_send()
                row_copy(offset, st).wait_send()

    finish_block(0)
    finish_block(2)
    add_slot(1, jnp.int32(SLOTS - 1))
    finish_block(1)
    finish_block(3)

    @pl.loop(0, SLOTS)
    def _(n):
        z_copy(1, 0, n).wait_send()
        z_copy(1, 1, n).wait_send()

    @pl.loop(0, BLOCKS + 2 * SLOTS)
    def _(n):
        d_copy(1, n, z, 0, core).wait_send()

    for b in range(BLOCKS):
        out_copy(b).wait()


def per_device(
    tokens,
    w_query,
    w_key,
    w_value,
    w_mem_query,
    w_mem_key,
    w_mem_value,
    w_gate,
    w_lift,
    decay_rate,
    store,
    passage_ids,
):
    cos_table, sin_table = rotary_tables()
    hbm = pl.BlockSpec(memory_space=pl.ANY)
    smem = pl.BlockSpec(memory_space=pltpu.SMEM)
    dma = pltpu.SemaphoreType.DMA
    return pl.pallas_call(
        kernel,
        out_shape=jax.ShapeDtypeStruct((SEQ_LEN, VALUE_DIM), BF16),
        in_specs=[hbm] * 12 + [smem] * 2,
        out_specs=hbm,
        scratch_shapes=[
            pltpu.VMEM((2, RING, BLOCKS, 2, BLOCK, HALF), BF16),
            pltpu.VMEM((D, TOK_COLS), BF16),
            pltpu.VMEM((D, 2 * MEM_DIM), BF16),
            pltpu.VMEM(store.shape, BF16),
            pltpu.VMEM((N_ST, PASS_ROWS, HALF), BF16),
            pltpu.VMEM((N_ST, PASS_ROWS, HALF), BF16),
            pltpu.VMEM((BLOCKS, BLOCK, TOK_COLS), F32),
            pltpu.VMEM((BLOCKS, BLOCK, 128), F32),
            pltpu.VMEM((BLOCKS, BLOCK, 128), F32),
            pltpu.VMEM((BLOCKS, BLOCK, 2 * MEM_DIM), F32),
            pltpu.VMEM((SEQ_LEN, KEY_DIM), BF16),
            pltpu.VMEM((SEQ_LEN, VALUE_DIM), BF16),
            pltpu.VMEM((BLOCKS, BLOCK, MEM_DIM), BF16),
            pltpu.VMEM((BLOCKS, BLOCK, 128), F32),
            pltpu.VMEM((BLOCKS, BLOCK, VALUE_DIM), F32),
            pltpu.VMEM((1, D), BF16),
            pltpu.VMEM((RING, 1, 512), F32),
            pltpu.VMEM((1, MEM_DIM, VALUE_DIM), BF16),
            pltpu.VMEM((SEQ_LEN, KEY_DIM), F32),
            pltpu.VMEM((SEQ_LEN, KEY_DIM), F32),
            pltpu.VMEM((BLOCKS, BLOCK, VALUE_DIM), BF16),
            pltpu.SMEM((N_ST, PICKS, BLOCKS), jnp.int32),
            dma((BLOCKS,)),
            dma((11,)),
            dma((BLOCKS,)),
            dma((2, 2, SLOTS)),
            dma((2, 2, SLOTS)),
            dma((2, BLOCKS + 2 * SLOTS)),
            dma((2, BLOCKS + 2 * SLOTS)),
            dma((N_ST,)),
            dma((N_ST,)),
            dma((N_ST,)),
            dma((N_ST,)),
        ],
        compiler_params=pltpu.CompilerParams(
            collective_id=0, has_side_effects=True, vmem_limit_bytes=67043328
        ),
        name="fused_layer",
    )(
        tokens,
        w_query,
        w_key,
        w_value,
        w_mem_query,
        w_mem_key,
        w_mem_value,
        w_gate.reshape(1, D),
        w_lift,
        store,
        cos_table,
        sin_table,
        decay_rate,
        passage_ids.T,
    )


def solution(mesh):
    in_specs = (
        P("st", "tp"),
        P(None, "tp"),
        P(None, "tp"),
        P(None, "tp"),
        P(None, "tp"),
        P(None, "tp"),
        P(None, "tp"),
        P(None, "tp"),
        P("tp", None, None),
        P("tp"),
        P("st", None, "tp"),
        P("st", None),
    )
    out_specs = P("st", "tp")
    return jax.shard_map(
        per_device, mesh=mesh, in_specs=in_specs, out_specs=out_specs, check_vma=False
    )
```

```python
import jax
import jax.numpy as jnp
import numpy as np
from jax import lax
from jax.experimental import pallas as pl
from jax.experimental.pallas import tpu as pltpu
from jax.sharding import PartitionSpec as P

D = 4096
KEY_DIM = 128
VALUE_DIM = 256
MEM_DIM = 128
SEQ_LEN = 512
BLOCK = 128
PICKS = 2
PASS_ROWS = 64
PASS_SHIFT = 7
N_ST = 16
RING = 8
BLOCKS = 4
SLOTS = 14
HALF = 256
TOK_COLS = 640

norm_eps = 1e-06
rope_base = 10000.0

F32 = jnp.float32
BF16 = jnp.bfloat16
MESH = pl.DeviceIdType.MESH


def rotary_tables():
    half = KEY_DIM // 2
    inverse = rope_base ** (-np.arange(half, dtype=np.float64) / half)
    angles = np.arange(SEQ_LEN, dtype=np.float64)[:, None] * inverse[None, :]
    cosine, sine = np.cos(angles), np.sin(angles)
    cos_table = np.concatenate([cosine, cosine], axis=1).astype(np.float32)
    sin_table = np.concatenate([-sine, sine], axis=1).astype(np.float32)
    return cos_table, sin_table


def dot(a, b):
    return jnp.dot(a, b, preferred_element_type=F32)


def dot_t(a, b):
    return lax.dot_general(a, b, (((1,), (1,)), ((), ())), preferred_element_type=F32)


def kernel(
    decay,
    tok,
    wq,
    wk,
    wv,
    wmq,
    wmk,
    wmv,
    wg,
    wl,
    store,
    cos_in,
    sin_in,
    ids_in,
    out,
    x,
    wt,
    wm,
    store_v,
    outbox,
    inbox,
    acc,
    squares,
    gates,
    acc_p,
    key_v,
    value_v,
    mem_q,
    gate_v,
    ret_norm,
    wg_v,
    wg_f,
    wl_v,
    cos_v,
    sin_v,
    ids,
    ids_all,
    tok_sem,
    local_sem,
    z_send,
    z_recv,
    d_send,
    d_recv,
    i_send,
    i_recv,
    s_send,
    s_recv,
):
    st = lax.axis_index("st")
    tp = lax.axis_index("tp")
    z = lax.div(tp, 2)
    core = lax.rem(tp, 2)
    other = 1 - core
    up = lax.rem(z + 1, RING) * 2 + core
    down = lax.rem(z + RING - 1, RING) * 2 + core
    partner = z * 2 + other

    def peer(offset):
        return lax.rem(st + offset, N_ST)

    tok_copies = [
        pltpu.make_async_copy(
            tok.at[pl.ds(b * BLOCK, BLOCK), :], x.at[0, z, b, core], tok_sem.at[b]
        )
        for b in range(BLOCKS)
    ]
    for copy in tok_copies:
        copy.start()
    local = [
        (ids_in, ids),
        (wg, wg_v),
        (wq, wt.at[:, pl.ds(0, 128)]),
        (wk, wt.at[:, pl.ds(128, 128)]),
        (wv, wt.at[:, pl.ds(256, 256)]),
        (wmq, wt.at[:, pl.ds(512, 128)]),
        (store, store_v),
        (wmk, wm.at[:, pl.ds(0, 128)]),
        (wmv, wm.at[:, pl.ds(128, 128)]),
        (wl, wl_v),
        (cos_in, cos_v),
        (sin_in, sin_v),
    ]
    local_copies = [
        pltpu.make_async_copy(src, dst, local_sem.at[i]) for i, (src, dst) in enumerate(local)
    ]
    local_copies[0].start()

    barrier = pltpu.get_barrier_semaphore()
    for target in (up, down, partner):
        pl.semaphore_signal(barrier, inc=1, device_id={"tp": target}, device_id_type=MESH)

    @pl.loop(1, N_ST)
    def _(offset):
        pl.semaphore_signal(
            barrier, inc=1, device_id={"st": peer(offset)}, device_id_type=MESH
        )

    pl.semaphore_wait(barrier, 3 + N_ST - 1)

    def slot_block(d, s):
        return lax.rem(s + 2 * d, BLOCKS)

    def chunk_at(d, hops):
        return lax.rem(z + RING - hops, RING) if d == 0 else lax.rem(z + hops, RING)

    def z_copy(phase, d, s):
        ref = x.at[phase, chunk_at(d, lax.div(s, BLOCKS)), slot_block(d, s), core]
        return pltpu.make_async_remote_copy(
            src_ref=ref,
            dst_ref=ref,
            send_sem=z_send.at[phase, d, s],
            recv_sem=z_recv.at[phase, d, s],
            device_id={"tp": up if d == 0 else down},
            device_id_type=MESH,
        )

    def z_arrival(phase, d, s):
        ref = x.at[phase, chunk_at(d, lax.div(s, BLOCKS) + 1), slot_block(d, s), core]
        return pltpu.make_async_remote_copy(
            src_ref=ref,
            dst_ref=ref,
            send_sem=z_send.at[phase, d, s],
            recv_sem=z_recv.at[phase, d, s],
            device_id={"tp": up if d == 0 else down},
            device_id_type=MESH,
        )

    def d_copy(phase, index, chunk, b, half):
        ref = x.at[phase, chunk, b, half]
        return pltpu.make_async_remote_copy(
            src_ref=ref,
            dst_ref=ref,
            send_sem=d_send.at[phase, index],
            recv_sem=d_recv.at[phase, index],
            device_id={"tp": partner},
            device_id_type=MESH,
        )

    def d_slot(d, s):
        return BLOCKS + d * SLOTS + s

    def send_own(phase):
        for b in range(BLOCKS):
            z_copy(phase, 0, jnp.int32(b)).start()
            z_copy(phase, 1, jnp.int32(b)).start()
        for b in range(BLOCKS):
            d_copy(phase, b, z, b, core).start()

    for copy in tok_copies:
        copy.wait()
    send_own(0)
    for copy in local_copies[1:]:
        copy.start()

    def id_copy(offset):
        return pltpu.make_async_remote_copy(
            src_ref=ids,
            dst_ref=ids_all.at[st],
            send_sem=i_send.at[offset],
            recv_sem=i_recv.at[offset],
            device_id={"st": peer(offset)},
            device_id_type=MESH,
        )

    local_copies[0].wait()

    @pl.loop(1, N_ST)
    def _(offset):
        id_copy(offset).start()

    local_copies[1].wait()
    for chunk in range(RING):
        wg_f[chunk] = wg_v[:, chunk * 512 : (chunk + 1) * 512].astype(F32)
    for copy in local_copies[2:]:
        copy.wait()

    def add_tokens(chunk, b, first=False):
        both = jnp.concatenate([x[0, chunk, b, 0], x[0, chunk, b, 1]], axis=1)
        rows = pl.ds(pl.multiple_of(chunk * 512, 512), 512)
        product = dot(both, wt[rows, :])
        wide = both.astype(F32)
        square = wide * wide
        gated = wide * wg_f[chunk]
        square = (square[:, 0:128] + square[:, 128:256]) + (
            square[:, 256:384] + square[:, 384:512]
        )
        gated = (gated[:, 0:128] + gated[:, 128:256]) + (gated[:, 256:384] + gated[:, 384:512])
        if first:
            acc[b] = product
            squares[b] = square
            gates[b] = gated
        else:
            acc[b] += product
            squares[b] += square
            gates[b] += gated

    def add_passages(chunk, b, first=False):
        both = jnp.concatenate([x[1, chunk, b, 0], x[1, chunk, b, 1]], axis=1)
        rows = pl.ds(pl.multiple_of(chunk * 512, 512), 512)
        product = dot(both, wm[rows, :])
        if first:
            acc_p[b] = product
        else:
            acc_p[b] += product

    def take_slot(phase, s, relay):
        for d in range(2):
            z_arrival(phase, d, s).wait_recv()
            if relay is True:
                z_copy(phase, d, s + BLOCKS).start()
            elif relay is not False:

                @pl.when(relay)
                def _():
                    z_copy(phase, d, s + BLOCKS).start()

            chunk = chunk_at(d, lax.div(s, BLOCKS) + 1)
            d_copy(phase, d_slot(d, s), chunk, slot_block(d, s), core).start()

    def add_slot(phase, s):
        for d in range(2):
            chunk = chunk_at(d, lax.div(s, BLOCKS) + 1)
            b = slot_block(d, s)
            d_copy(phase, d_slot(d, s), chunk, b, other).wait_recv()
            if phase == 0:
                add_tokens(chunk, b)
            else:
                add_passages(chunk, b)

    for b in range(BLOCKS):
        d_copy(0, b, z, b, other).wait_recv()
        add_tokens(z, b, first=True)

    def id_arrival(offset):
        return pltpu.make_async_remote_copy(
            src_ref=ids,
            dst_ref=ids_all.at[peer(N_ST - offset)],
            send_sem=i_send.at[offset],
            recv_sem=i_recv.at[offset],
            device_id={"st": peer(offset)},
            device_id_type=MESH,
        )

    take_slot(0, jnp.int32(0), True)

    @pl.loop(1, N_ST)
    def _(offset):
        id_arrival(offset).wait_recv()

    def wanted_row(read):
        row = jnp.int32(0)
        for pick in range(PICKS):
            for b in range(BLOCKS):
                ident = read(pick, b)
                mine = lax.shift_right_logical(ident, PASS_SHIFT) == st
                row = row + jnp.where(mine, ident & ((1 << PASS_SHIFT) - 1), 0)
        return row

    inbox[st] = store_v[wanted_row(lambda pick, b: ids[pick, b])]

    @pl.loop(1, N_ST)
    def _(offset):
        target = peer(offset)
        outbox[offset] = store_v[wanted_row(lambda pick, b: ids_all[target, pick, b])]

    take_slot(0, jnp.int32(1), True)
    add_slot(0, jnp.int32(0))

    def row_copy(offset, place):
        return pltpu.make_async_remote_copy(
            src_ref=outbox.at[offset],
            dst_ref=inbox.at[place],
            send_sem=s_send.at[offset],
            recv_sem=s_recv.at[offset],
            device_id={"st": peer(offset)},
            device_id_type=MESH,
        )

    @pl.loop(1, N_ST)
    def _(offset):
        row_copy(offset, st).start()

    @pl.loop(2, 9)
    def _(s):
        take_slot(0, s, True)
        add_slot(0, s - 1)

    @pl.loop(1, N_ST)
    def _(offset):
        row_copy(offset, peer(N_ST - offset)).wait_recv()

    for b in range(BLOCKS):
        for pick in range(PICKS):
            owner = lax.shift_right_logical(ids[pick, b], PASS_SHIFT)
            x[1, z, b, core, pick * PASS_ROWS : (pick + 1) * PASS_ROWS, :] = inbox[owner]

    take_slot(0, jnp.int32(9), True)
    add_slot(0, jnp.int32(8))
    send_own(1)

    @pl.loop(10, SLOTS)
    def _(s):
        take_slot(0, s, False)
        add_slot(0, s - 1)

    rate = decay[0]

    def finish_tokens(b):
        mean_square = jnp.sum(squares[b], axis=1, keepdims=True) * (1.0 / D)
        scale = lax.rsqrt(mean_square + norm_eps)
        cosine = cos_v[b * BLOCK : (b + 1) * BLOCK, :]
        sine = sin_v[b * BLOCK : (b + 1) * BLOCK, :]

        def rotate(values):
            return values * cosine + pltpu.roll(values, KEY_DIM // 2, 1) * sine

        query = rotate(acc[b, :, 0:128] * scale).astype(BF16)
        key = (rotate(acc[b, :, 128:256] * scale) * KEY_DIM ** (-0.5)).astype(BF16)
        key_v[b * BLOCK : (b + 1) * BLOCK, :] = key
        value_v[b * BLOCK : (b + 1) * BLOCK, :] = (acc[b, :, 256:512] * scale).astype(BF16)
        memory = acc[b, :, 512:640]
        mean = jnp.mean(memory * memory, axis=1, keepdims=True)
        mem_q[b] = (memory * lax.rsqrt(mean + norm_eps)).astype(BF16)
        gate = jnp.sum(gates[b], axis=1, keepdims=True) * scale
        gate_v[b] = jnp.broadcast_to(jax.nn.sigmoid(gate), (BLOCK, 128))

        span = (b + 1) * BLOCK
        keys = key_v[0:span, :]
        values = value_v[0:span, :]
        row = lax.broadcasted_iota(jnp.int32, (BLOCK, span), 0) + b * BLOCK
        column = lax.broadcasted_iota(jnp.int32, (BLOCK, span), 1)
        distance = (row - column).astype(F32)
        mask = jnp.where(distance >= 0.0, jnp.exp(-rate * jnp.maximum(distance, 0.0)), 0.0)
        scores = dot_t(query, keys) * mask
        upper = scores.astype(BF16)
        lower = (scores - upper.astype(F32)).astype(BF16)
        mixed = dot(upper, values) + dot(lower, values)
        centred = mixed - jnp.mean(mixed, axis=1, keepdims=True)
        variance = jnp.mean(centred * centred, axis=1, keepdims=True)
        ret_norm[b] = centred * lax.rsqrt(variance + norm_eps)

    def finish_block(b):
        raw = acc_p[b, :, 0:128]
        mean = jnp.mean(raw * raw, axis=1, keepdims=True)
        pass_key = (raw * lax.rsqrt(mean + norm_eps)).astype(BF16)
        pass_value = acc_p[b, :, 128:256].astype(BF16)
        exponent = jnp.exp(dot_t(mem_q[b], pass_key) * MEM_DIM ** (-0.5))
        mass = jnp.sum(exponent, axis=1, keepdims=True)
        summed = dot(exponent.astype(BF16), pass_value)
        mem_out = (summed / mass).astype(BF16)
        lift = dot(mem_out, wl_v[0])
        gate = gate_v[b]
        gate = jnp.concatenate([gate, gate], axis=1)
        out[b * BLOCK : (b + 1) * BLOCK, :] = (ret_norm[b] + gate * lift).astype(BF16)

    for s in range(SLOTS):
        take_slot(1, jnp.int32(s), s < SLOTS - BLOCKS)
        if s == 0:
            add_slot(0, jnp.int32(SLOTS - 1))
            for b in range(BLOCKS):
                d_copy(1, b, z, b, other).wait_recv()
                add_passages(z, b, first=True)
        else:
            add_slot(1, jnp.int32(s - 1))
        if s < BLOCKS:
            finish_tokens(s)
        if s == 8:

            @pl.loop(0, SLOTS)
            def _(n):
                z_copy(0, 0, n).wait_send()
                z_copy(0, 1, n).wait_send()

            @pl.loop(0, BLOCKS + 2 * SLOTS)
            def _(n):
                d_copy(0, n, z, 0, core).wait_send()

            @pl.loop(1, N_ST)
            def _(offset):
                id_copy(offset).wait_send()
                row_copy(offset, st).wait_send()

    finish_block(0)
    finish_block(2)
    add_slot(1, jnp.int32(SLOTS - 1))
    finish_block(1)
    finish_block(3)

    @pl.loop(0, SLOTS)
    def _(n):
        z_copy(1, 0, n).wait_send()
        z_copy(1, 1, n).wait_send()

    @pl.loop(0, BLOCKS + 2 * SLOTS)
    def _(n):
        d_copy(1, n, z, 0, core).wait_send()


def per_device(
    tokens,
    w_query,
    w_key,
    w_value,
    w_mem_query,
    w_mem_key,
    w_mem_value,
    w_gate,
    w_lift,
    decay_rate,
    store,
    passage_ids,
):
    cos_table, sin_table = rotary_tables()
    hbm = pl.BlockSpec(memory_space=pltpu.HBM)
    dma = pltpu.SemaphoreType.DMA
    operands = (
        tokens,
        w_query,
        w_key,
        w_value,
        w_mem_query,
        w_mem_key,
        w_mem_value,
        w_gate.reshape(1, D),
        w_lift,
        store,
        jnp.asarray(cos_table),
        jnp.asarray(sin_table),
        passage_ids.T,
    )
    return pl.pallas_call(
        kernel,
        out_shape=pltpu.VMEM((SEQ_LEN, VALUE_DIM), BF16),
        in_specs=[pl.BlockSpec(memory_space=pltpu.SMEM)] + [hbm] * 13,
        out_specs=pl.BlockSpec(memory_space=pltpu.VMEM),
        scratch_shapes=[
            pltpu.VMEM((2, RING, BLOCKS, 2, BLOCK, HALF), BF16),
            pltpu.VMEM((D, TOK_COLS), BF16),
            pltpu.VMEM((D, 2 * MEM_DIM), BF16),
            pltpu.VMEM(store.shape, BF16),
            pltpu.VMEM((N_ST, PASS_ROWS, HALF), BF16),
            pltpu.VMEM((N_ST, PASS_ROWS, HALF), BF16),
            pltpu.VMEM((BLOCKS, BLOCK, TOK_COLS), F32),
            pltpu.VMEM((BLOCKS, BLOCK, 128), F32),
            pltpu.VMEM((BLOCKS, BLOCK, 128), F32),
            pltpu.VMEM((BLOCKS, BLOCK, 2 * MEM_DIM), F32),
            pltpu.VMEM((SEQ_LEN, KEY_DIM), BF16),
            pltpu.VMEM((SEQ_LEN, VALUE_DIM), BF16),
            pltpu.VMEM((BLOCKS, BLOCK, MEM_DIM), BF16),
            pltpu.VMEM((BLOCKS, BLOCK, 128), F32),
            pltpu.VMEM((BLOCKS, BLOCK, VALUE_DIM), F32),
            pltpu.VMEM((1, D), BF16),
            pltpu.VMEM((RING, 1, 512), F32),
            pltpu.VMEM((1, MEM_DIM, VALUE_DIM), BF16),
            pltpu.VMEM((SEQ_LEN, KEY_DIM), F32),
            pltpu.VMEM((SEQ_LEN, KEY_DIM), F32),
            pltpu.SMEM((PICKS, BLOCKS), jnp.int32),
            pltpu.SMEM((N_ST, PICKS, BLOCKS), jnp.int32),
            dma((BLOCKS,)),
            dma((12,)),
            dma((2, 2, SLOTS)),
            dma((2, 2, SLOTS)),
            dma((2, BLOCKS + 2 * SLOTS)),
            dma((2, BLOCKS + 2 * SLOTS)),
            dma((N_ST,)),
            dma((N_ST,)),
            dma((N_ST,)),
            dma((N_ST,)),
        ],
        compiler_params=pltpu.CompilerParams(
            collective_id=0, has_side_effects=True, vmem_limit_bytes=48 * 1024 * 1024
        ),
        name="fused_layer",
    )(decay_rate, *[pltpu.with_memory_space_constraint(array, pltpu.HBM) for array in operands])


def solution(mesh):
    in_specs = (
        P("st", "tp"),
        P(None, "tp"),
        P(None, "tp"),
        P(None, "tp"),
        P(None, "tp"),
        P(None, "tp"),
        P(None, "tp"),
        P(None, "tp"),
        P("tp", None, None),
        P("tp"),
        P("st", None, "tp"),
        P("st", None),
    )
    out_specs = P("st", "tp")
    return jax.shard_map(
        per_device, mesh=mesh, in_specs=in_specs, out_specs=out_specs, check_vma=False
    )
```

```python
import jax
import jax.numpy as jnp
import numpy as np
from jax import lax
from jax.experimental import pallas as pl
from jax.experimental.pallas import tpu as pltpu
from jax.sharding import PartitionSpec as P

D = 4096
KEY_DIM = 128
VALUE_DIM = 256
MEM_DIM = 128
SEQ_LEN = 512
BLOCK = 128
PICKS = 2
PASS_ROWS = 64
PASS_SHIFT = 7
N_ST = 16
RING = 8
BLOCKS = 4
SLOTS = 14
HALF = 256
TOK_COLS = 640

STEPS = sorted(
    ((a, b) for a in range(4) for b in range(4) if a or b),
    key=lambda step: sum(min(part, 4 - part) for part in step),
)
RINGS = [range(0, 4), range(4, 10), range(10, 14), range(14, 15)]

norm_eps = 1e-06
rope_base = 10000.0

F32 = jnp.float32
BF16 = jnp.bfloat16
MESH = pl.DeviceIdType.MESH


def rotary_tables():
    half = KEY_DIM // 2
    inverse = rope_base ** (-np.arange(half, dtype=np.float64) / half)
    angles = np.arange(SEQ_LEN, dtype=np.float64)[:, None] * inverse[None, :]
    cosine, sine = np.cos(angles), np.sin(angles)
    cos_table = np.concatenate([cosine, cosine], axis=1).astype(np.float32)
    sin_table = np.concatenate([-sine, sine], axis=1).astype(np.float32)
    return cos_table, sin_table


def dot(a, b):
    return jnp.dot(a, b, preferred_element_type=F32)


def dot_t(a, b):
    return lax.dot_general(a, b, (((1,), (1,)), ((), ())), preferred_element_type=F32)


def kernel(
    decay,
    tok,
    wq,
    wk,
    wv,
    wmq,
    wmk,
    wmv,
    wg,
    wl,
    store,
    cos_in,
    sin_in,
    ids_in,
    out,
    x,
    wt,
    wm,
    store_v,
    outbox,
    inbox,
    acc,
    squares,
    gates,
    acc_p,
    key_v,
    value_v,
    mem_q,
    gate_v,
    ret_norm,
    wg_v,
    wg_f,
    wl_v,
    cos_v,
    sin_v,
    ids,
    ids_all,
    tok_sem,
    local_sem,
    z_send,
    z_recv,
    d_send,
    d_recv,
    i_send,
    i_recv,
    s_send,
    s_recv,
    meet_sem,
):
    st = lax.axis_index("st")
    tp = lax.axis_index("tp")
    z = lax.div(tp, 2)
    core = lax.rem(tp, 2)
    other = 1 - core
    up = lax.rem(z + 1, RING) * 2 + core
    down = lax.rem(z + RING - 1, RING) * 2 + core
    partner = z * 2 + other

    side = 4
    row, column = lax.div(st, side), lax.rem(st, side)

    def peer(place):
        down_by, right_by = STEPS[place]
        return lax.rem(row + down_by, side) * side + lax.rem(column + right_by, side)

    def source(place):
        down_by, right_by = STEPS[place]
        return lax.rem(row + side - down_by, side) * side + lax.rem(
            column + side - right_by, side
        )

    near = [peer(place) for place in RINGS[0]]

    tok_copies = [
        pltpu.make_async_copy(
            tok.at[pl.ds(b * BLOCK, BLOCK), :], x.at[0, z, b, core], tok_sem.at[b]
        )
        for b in range(BLOCKS)
    ]
    for copy in tok_copies:
        copy.start()
    local = [
        (ids_in, ids),
        (store, store_v),
        (wg, wg_v),
        (wq, wt.at[:, pl.ds(0, 128)]),
        (wk, wt.at[:, pl.ds(128, 128)]),
        (wv, wt.at[:, pl.ds(256, 256)]),
        (wmq, wt.at[:, pl.ds(512, 128)]),
        (wmk, wm.at[:, pl.ds(0, 128)]),
        (wmv, wm.at[:, pl.ds(128, 128)]),
        (wl, wl_v),
        (cos_in, cos_v),
        (sin_in, sin_v),
    ]
    local_copies = [
        pltpu.make_async_copy(src, dst, local_sem.at[i]) for i, (src, dst) in enumerate(local)
    ]
    local_copies[0].start()

    barrier = pltpu.get_barrier_semaphore()
    for target in (up, down, partner):
        pl.semaphore_signal(barrier, inc=1, device_id={"tp": target}, device_id_type=MESH)
    for target in near:
        pl.semaphore_signal(barrier, inc=1, device_id={"st": target}, device_id_type=MESH)
    pl.semaphore_wait(barrier, 3 + len(near))

    def tell(step):
        for target in near:
            pl.semaphore_signal(
                meet_sem.at[step], inc=1, device_id={"st": target}, device_id_type=MESH
            )

    def meet(step):
        pl.semaphore_wait(meet_sem.at[step], len(near))

    tell(0)

    def slot_block(d, s):
        return lax.rem(s + 2 * d, BLOCKS)

    def chunk_at(d, hops):
        return lax.rem(z + RING - hops, RING) if d == 0 else lax.rem(z + hops, RING)

    def z_copy(phase, d, s):
        ref = x.at[phase, chunk_at(d, lax.div(s, BLOCKS)), slot_block(d, s), core]
        return pltpu.make_async_remote_copy(
            src_ref=ref,
            dst_ref=ref,
            send_sem=z_send.at[phase, d, s],
            recv_sem=z_recv.at[phase, d, s],
            device_id={"tp": up if d == 0 else down},
            device_id_type=MESH,
        )

    def z_arrival(phase, d, s):
        ref = x.at[phase, chunk_at(d, lax.div(s, BLOCKS) + 1), slot_block(d, s), core]
        return pltpu.make_async_remote_copy(
            src_ref=ref,
            dst_ref=ref,
            send_sem=z_send.at[phase, d, s],
            recv_sem=z_recv.at[phase, d, s],
            device_id={"tp": up if d == 0 else down},
            device_id_type=MESH,
        )

    def d_copy(phase, index, chunk, b, half):
        ref = x.at[phase, chunk, b, half]
        return pltpu.make_async_remote_copy(
            src_ref=ref,
            dst_ref=ref,
            send_sem=d_send.at[phase, index],
            recv_sem=d_recv.at[phase, index],
            device_id={"tp": partner},
            device_id_type=MESH,
        )

    def d_slot(d, s):
        return BLOCKS + d * SLOTS + s

    def send_own(phase):
        for b in range(BLOCKS):
            z_copy(phase, 0, jnp.int32(b)).start()
            z_copy(phase, 1, jnp.int32(b)).start()
        for b in range(BLOCKS):
            d_copy(phase, b, z, b, core).start()

    for copy in tok_copies:
        copy.wait()
    send_own(0)
    for copy in local_copies[1:]:
        copy.start()

    def id_copy(place, slot):
        return pltpu.make_async_remote_copy(
            src_ref=ids,
            dst_ref=ids_all.at[slot],
            send_sem=i_send.at[place],
            recv_sem=i_recv.at[place],
            device_id={"st": peer(place)},
            device_id_type=MESH,
        )

    def row_copy(place, slot):
        return pltpu.make_async_remote_copy(
            src_ref=outbox.at[place],
            dst_ref=inbox.at[slot],
            send_sem=s_send.at[place],
            recv_sem=s_recv.at[place],
            device_id={"st": peer(place)},
            device_id_type=MESH,
        )

    def wanted_row(read):
        wanted = jnp.int32(0)
        for pick in range(PICKS):
            for b in range(BLOCKS):
                ident = read(pick, b)
                mine = lax.shift_right_logical(ident, PASS_SHIFT) == st
                wanted = wanted + jnp.where(mine, ident & ((1 << PASS_SHIFT) - 1), 0)
        return wanted

    def send_ids(ring):
        for place in RINGS[ring]:
            id_copy(place, st).start()

    def gather_rows(ring):
        for place in RINGS[ring]:
            id_copy(place, source(place)).wait_recv()
        for place in RINGS[ring]:
            target = peer(place)
            outbox[place] = store_v[wanted_row(lambda pick, b: ids_all[target, pick, b])]

    def send_rows(ring):
        for place in RINGS[ring]:
            row_copy(place, st).start()

    def add_tokens(chunk, b, first=False):
        both = jnp.concatenate([x[0, chunk, b, 0], x[0, chunk, b, 1]], axis=1)
        rows = pl.ds(pl.multiple_of(chunk * 512, 512), 512)
        product = dot(both, wt[rows, :])
        wide = both.astype(F32)
        square = wide * wide
        gated = wide * wg_f[chunk]
        square = (square[:, 0:128] + square[:, 128:256]) + (
            square[:, 256:384] + square[:, 384:512]
        )
        gated = (gated[:, 0:128] + gated[:, 128:256]) + (gated[:, 256:384] + gated[:, 384:512])
        if first:
            acc[b] = product
            squares[b] = square
            gates[b] = gated
        else:
            acc[b] += product
            squares[b] += square
            gates[b] += gated

    def add_passages(chunk, b, first=False):
        both = jnp.concatenate([x[1, chunk, b, 0], x[1, chunk, b, 1]], axis=1)
        rows = pl.ds(pl.multiple_of(chunk * 512, 512), 512)
        product = dot(both, wm[rows, :])
        if first:
            acc_p[b] = product
        else:
            acc_p[b] += product

    def take_slot(phase, s, relay):
        for d in range(2):
            z_arrival(phase, d, s).wait_recv()
            if relay is True:
                z_copy(phase, d, s + BLOCKS).start()
            elif relay is not False:

                @pl.when(relay)
                def _():
                    z_copy(phase, d, s + BLOCKS).start()

            chunk = chunk_at(d, lax.div(s, BLOCKS) + 1)
            d_copy(phase, d_slot(d, s), chunk, slot_block(d, s), core).start()

    def add_slot(phase, s):
        for d in range(2):
            chunk = chunk_at(d, lax.div(s, BLOCKS) + 1)
            b = slot_block(d, s)
            d_copy(phase, d_slot(d, s), chunk, b, other).wait_recv()
            if phase == 0:
                add_tokens(chunk, b)
            else:
                add_passages(chunk, b)

    def add_own_tokens(b):
        d_copy(0, b, z, b, other).wait_recv()
        add_tokens(z, b, first=True)

    def take(s):
        take_slot(0, jnp.int32(s), True)

    def add(s):
        add_slot(0, jnp.int32(s))

    local_copies[0].wait()
    send_ids(0)
    meet(0)
    tell(1)
    send_ids(1)
    take(0)
    meet(1)
    tell(2)
    send_ids(2)
    take(1)
    meet(2)
    send_ids(3)
    local_copies[1].wait()
    inbox[st] = store_v[wanted_row(lambda pick, b: ids[pick, b])]
    take(2)
    gather_rows(0)
    take(3)
    send_rows(0)
    gather_rows(1)
    take(4)
    send_rows(1)
    gather_rows(2)
    take(5)
    send_rows(2)
    gather_rows(3)
    for copy in local_copies[2:]:
        copy.wait()
    for chunk in range(RING):
        wg_f[chunk] = wg_v[:, chunk * 512 : (chunk + 1) * 512].astype(F32)
    add_own_tokens(0)
    add_own_tokens(1)
    take(6)
    send_rows(3)
    add_own_tokens(2)
    add_own_tokens(3)
    add(0)

    @pl.loop(7, 10)
    def _(s):
        take_slot(0, s, True)

        @pl.loop(0, jnp.where(s < 9, 3, 2))
        def _(n):
            add_slot(0, 1 + 3 * (s - 7) + n)

    for place in range(N_ST - 1):
        row_copy(place, source(place)).wait_recv()
    for b in range(BLOCKS):
        for pick in range(PICKS):
            owner = lax.shift_right_logical(ids[pick, b], PASS_SHIFT)
            x[1, z, b, core, pick * PASS_ROWS : (pick + 1) * PASS_ROWS, :] = inbox[owner]

    add_slot(0, jnp.int32(9))
    send_own(1)

    @pl.loop(10, SLOTS)
    def _(s):
        take_slot(0, s, False)

        @pl.when(s > 10)
        def _():
            add_slot(0, s - 1)

    rate = decay[0]

    def finish_tokens(b):
        mean_square = jnp.sum(squares[b], axis=1, keepdims=True) * (1.0 / D)
        scale = lax.rsqrt(mean_square + norm_eps)
        cosine = cos_v[b * BLOCK : (b + 1) * BLOCK, :]
        sine = sin_v[b * BLOCK : (b + 1) * BLOCK, :]

        def rotate(values):
            return values * cosine + pltpu.roll(values, KEY_DIM // 2, 1) * sine

        query = rotate(acc[b, :, 0:128] * scale).astype(BF16)
        key = (rotate(acc[b, :, 128:256] * scale) * KEY_DIM ** (-0.5)).astype(BF16)
        key_v[b * BLOCK : (b + 1) * BLOCK, :] = key
        value_v[b * BLOCK : (b + 1) * BLOCK, :] = (acc[b, :, 256:512] * scale).astype(BF16)
        memory = acc[b, :, 512:640]
        mean = jnp.mean(memory * memory, axis=1, keepdims=True)
        mem_q[b] = (memory * lax.rsqrt(mean + norm_eps)).astype(BF16)
        gate = jnp.sum(gates[b], axis=1, keepdims=True) * scale
        gate_v[b] = jnp.broadcast_to(jax.nn.sigmoid(gate), (BLOCK, 128))

        span = (b + 1) * BLOCK
        keys = key_v[0:span, :]
        values = value_v[0:span, :]
        row = lax.broadcasted_iota(jnp.int32, (BLOCK, span), 0) + b * BLOCK
        column = lax.broadcasted_iota(jnp.int32, (BLOCK, span), 1)
        distance = (row - column).astype(F32)
        mask = jnp.where(distance >= 0.0, jnp.exp(-rate * jnp.maximum(distance, 0.0)), 0.0)
        scores = dot_t(query, keys) * mask
        upper = scores.astype(BF16)
        lower = (scores - upper.astype(F32)).astype(BF16)
        mixed = dot(upper, values) + dot(lower, values)
        centred = mixed - jnp.mean(mixed, axis=1, keepdims=True)
        variance = jnp.mean(centred * centred, axis=1, keepdims=True)
        ret_norm[b] = centred * lax.rsqrt(variance + norm_eps)

    def finish_block(b):
        raw = acc_p[b, :, 0:128]
        mean = jnp.mean(raw * raw, axis=1, keepdims=True)
        pass_key = (raw * lax.rsqrt(mean + norm_eps)).astype(BF16)
        pass_value = acc_p[b, :, 128:256].astype(BF16)
        exponent = jnp.exp(dot_t(mem_q[b], pass_key) * MEM_DIM ** (-0.5))
        mass = jnp.sum(exponent, axis=1, keepdims=True)
        summed = dot(exponent.astype(BF16), pass_value)
        mem_out = (summed / mass).astype(BF16)
        lift = dot(mem_out, wl_v[0])
        gate = gate_v[b]
        gate = jnp.concatenate([gate, gate], axis=1)
        out[b * BLOCK : (b + 1) * BLOCK, :] = (ret_norm[b] + gate * lift).astype(BF16)

    for s in range(SLOTS):
        take_slot(1, jnp.int32(s), s < SLOTS - BLOCKS)
        if s == 0:
            add_slot(0, jnp.int32(SLOTS - 1))
            for b in range(BLOCKS):
                d_copy(1, b, z, b, other).wait_recv()
                add_passages(z, b, first=True)
        else:
            add_slot(1, jnp.int32(s - 1))
        if s < BLOCKS:
            finish_tokens(s)
        if s == 8:

            @pl.loop(0, SLOTS)
            def _(n):
                z_copy(0, 0, n).wait_send()
                z_copy(0, 1, n).wait_send()

            @pl.loop(0, BLOCKS + 2 * SLOTS)
            def _(n):
                d_copy(0, n, z, 0, core).wait_send()

            for place in range(N_ST - 1):
                id_copy(place, st).wait_send()
                row_copy(place, st).wait_send()

    finish_block(0)
    finish_block(2)
    add_slot(1, jnp.int32(SLOTS - 1))
    finish_block(1)
    finish_block(3)

    @pl.loop(0, SLOTS)
    def _(n):
        z_copy(1, 0, n).wait_send()
        z_copy(1, 1, n).wait_send()

    @pl.loop(0, BLOCKS + 2 * SLOTS)
    def _(n):
        d_copy(1, n, z, 0, core).wait_send()


def per_device(
    tokens,
    w_query,
    w_key,
    w_value,
    w_mem_query,
    w_mem_key,
    w_mem_value,
    w_gate,
    w_lift,
    decay_rate,
    store,
    passage_ids,
):
    cos_table, sin_table = rotary_tables()
    hbm = pl.BlockSpec(memory_space=pltpu.HBM)
    dma = pltpu.SemaphoreType.DMA
    operands = (
        tokens,
        w_query,
        w_key,
        w_value,
        w_mem_query,
        w_mem_key,
        w_mem_value,
        w_gate.reshape(1, D),
        w_lift,
        store,
        jnp.asarray(cos_table),
        jnp.asarray(sin_table),
        passage_ids.T,
    )
    return pl.pallas_call(
        kernel,
        out_shape=pltpu.VMEM((SEQ_LEN, VALUE_DIM), BF16),
        in_specs=[pl.BlockSpec(memory_space=pltpu.SMEM)] + [hbm] * 13,
        out_specs=pl.BlockSpec(memory_space=pltpu.VMEM),
        scratch_shapes=[
            pltpu.VMEM((2, RING, BLOCKS, 2, BLOCK, HALF), BF16),
            pltpu.VMEM((D, TOK_COLS), BF16),
            pltpu.VMEM((D, 2 * MEM_DIM), BF16),
            pltpu.VMEM(store.shape, BF16),
            pltpu.VMEM((N_ST, PASS_ROWS, HALF), BF16),
            pltpu.VMEM((N_ST, PASS_ROWS, HALF), BF16),
            pltpu.VMEM((BLOCKS, BLOCK, TOK_COLS), F32),
            pltpu.VMEM((BLOCKS, BLOCK, 128), F32),
            pltpu.VMEM((BLOCKS, BLOCK, 128), F32),
            pltpu.VMEM((BLOCKS, BLOCK, 2 * MEM_DIM), F32),
            pltpu.VMEM((SEQ_LEN, KEY_DIM), BF16),
            pltpu.VMEM((SEQ_LEN, VALUE_DIM), BF16),
            pltpu.VMEM((BLOCKS, BLOCK, MEM_DIM), BF16),
            pltpu.VMEM((BLOCKS, BLOCK, 128), F32),
            pltpu.VMEM((BLOCKS, BLOCK, VALUE_DIM), F32),
            pltpu.VMEM((1, D), BF16),
            pltpu.VMEM((RING, 1, 512), F32),
            pltpu.VMEM((1, MEM_DIM, VALUE_DIM), BF16),
            pltpu.VMEM((SEQ_LEN, KEY_DIM), F32),
            pltpu.VMEM((SEQ_LEN, KEY_DIM), F32),
            pltpu.SMEM((PICKS, BLOCKS), jnp.int32),
            pltpu.SMEM((N_ST, PICKS, BLOCKS), jnp.int32),
            dma((BLOCKS,)),
            dma((12,)),
            dma((2, 2, SLOTS)),
            dma((2, 2, SLOTS)),
            dma((2, BLOCKS + 2 * SLOTS)),
            dma((2, BLOCKS + 2 * SLOTS)),
            dma((N_ST,)),
            dma((N_ST,)),
            dma((N_ST,)),
            dma((N_ST,)),
            pltpu.SemaphoreType.REGULAR((3,)),
        ],
        compiler_params=pltpu.CompilerParams(
            collective_id=0, has_side_effects=True, vmem_limit_bytes=48 * 1024 * 1024
        ),
        name="fused_layer",
    )(decay_rate, *[pltpu.with_memory_space_constraint(array, pltpu.HBM) for array in operands])


def solution(mesh):
    in_specs = (
        P("st", "tp"),
        P(None, "tp"),
        P(None, "tp"),
        P(None, "tp"),
        P(None, "tp"),
        P(None, "tp"),
        P(None, "tp"),
        P(None, "tp"),
        P("tp", None, None),
        P("tp"),
        P("st", None, "tp"),
        P("st", None),
    )
    out_specs = P("st", "tp")
    return jax.shard_map(
        per_device, mesh=mesh, in_specs=in_specs, out_specs=out_specs, check_vma=False
    )
```

```python
import jax
import jax.numpy as jnp
import numpy as np
from jax import lax
from jax.experimental import pallas as pl
from jax.experimental.pallas import tpu as pltpu
from jax.sharding import PartitionSpec as P

D = 4096
KEY_DIM = 128
VALUE_DIM = 256
MEM_DIM = 128
SEQ_LEN = 512
BLOCK = 128
PICKS = 2
PASS_ROWS = 64
PASS_SHIFT = 7
N_ST = 16
RING = 8
BLOCKS = 4
SLOTS = 14
PAIRS = SLOTS // 2
HALF = 256
TOK_COLS = 640

STEPS = sorted(
    ((a, b) for a in range(4) for b in range(4) if a or b),
    key=lambda step: sum(min(part, 4 - part) for part in step),
)
RINGS = [range(0, 4), range(4, 10), range(10, 14), range(14, 15)]

norm_eps = 1e-06
rope_base = 10000.0

F32 = jnp.float32
BF16 = jnp.bfloat16
MESH = pl.DeviceIdType.MESH


def rotary_tables():
    half = KEY_DIM // 2
    inverse = rope_base ** (-np.arange(half, dtype=np.float64) / half)
    angles = np.arange(SEQ_LEN, dtype=np.float64)[:, None] * inverse[None, :]
    cosine, sine = np.cos(angles), np.sin(angles)
    cos_table = np.concatenate([cosine, cosine], axis=1).astype(np.float32)
    sin_table = np.concatenate([-sine, sine], axis=1).astype(np.float32)
    return cos_table, sin_table


def dot(a, b):
    return jnp.dot(a, b, preferred_element_type=F32)


def dot_t(a, b):
    return lax.dot_general(a, b, (((1,), (1,)), ((), ())), preferred_element_type=F32)


def kernel(
    decay,
    tok,
    wq,
    wk,
    wv,
    wmq,
    wmk,
    wmv,
    wg,
    wl,
    store,
    cos_in,
    sin_in,
    ids_in,
    out,
    x,
    wt,
    wm,
    store_v,
    outbox,
    inbox,
    acc,
    squares,
    gates,
    acc_p,
    key_v,
    value_v,
    mem_q,
    gate_v,
    ret_norm,
    wg_v,
    wg_f,
    wl_v,
    cos_v,
    sin_v,
    ids,
    ids_all,
    tok_sem,
    local_sem,
    z_send,
    z_recv,
    d_send,
    d_recv,
    i_send,
    i_recv,
    s_send,
    s_recv,
    meet_sem,
):
    st = lax.axis_index("st")
    tp = lax.axis_index("tp")
    z = lax.div(tp, 2)
    core = lax.rem(tp, 2)
    other = 1 - core
    up = lax.rem(z + 1, RING) * 2 + core
    down = lax.rem(z + RING - 1, RING) * 2 + core
    partner = z * 2 + other

    side = 4
    row, column = lax.div(st, side), lax.rem(st, side)

    def peer(place):
        down_by, right_by = STEPS[place]
        return lax.rem(row + down_by, side) * side + lax.rem(column + right_by, side)

    def source(place):
        down_by, right_by = STEPS[place]
        return lax.rem(row + side - down_by, side) * side + lax.rem(
            column + side - right_by, side
        )

    near = (
        lax.rem(row + 1, side) * side + column,
        lax.rem(row + side - 1, side) * side + column,
        row * side + lax.rem(column + 1, side),
        row * side + lax.rem(column + side - 1, side),
    )

    tok_copies = [
        pltpu.make_async_copy(
            tok.at[pl.ds(b * BLOCK, BLOCK), :], x.at[0, z, core, b], tok_sem.at[b]
        )
        for b in range(BLOCKS)
    ]
    for copy in tok_copies:
        copy.start()
    local = [
        (ids_in, ids),
        (store, store_v),
        (wg, wg_v),
        (wq, wt.at[:, pl.ds(0, 128)]),
        (wk, wt.at[:, pl.ds(128, 128)]),
        (wv, wt.at[:, pl.ds(256, 256)]),
        (wmq, wt.at[:, pl.ds(512, 128)]),
        (wmk, wm.at[:, pl.ds(0, 128)]),
        (wmv, wm.at[:, pl.ds(128, 128)]),
        (wl, wl_v),
        (cos_in, cos_v),
        (sin_in, sin_v),
    ]
    local_copies = [
        pltpu.make_async_copy(src, dst, local_sem.at[i]) for i, (src, dst) in enumerate(local)
    ]
    local_copies[0].start()

    barrier = pltpu.get_barrier_semaphore()
    for target in (up, down, partner):
        pl.semaphore_signal(barrier, inc=1, device_id={"tp": target}, device_id_type=MESH)
    ahead = (row < side - 1, row == 0, column < side - 1, column == 0)
    behind = (row == side - 1, row > 0, column == side - 1, column > 0)
    for target, chosen in zip(near, ahead):

        @pl.when(chosen)
        def _():
            pl.semaphore_signal(barrier, inc=1, device_id={"st": target}, device_id_type=MESH)

    early = sum(one.astype(jnp.int32) for one in behind)
    pl.semaphore_wait(barrier, 3 + early)

    def tell(step):
        for target, chosen in zip(near, behind):

            def signal():
                pl.semaphore_signal(
                    meet_sem.at[step], inc=1, device_id={"st": target}, device_id_type=MESH
                )

            if step == 0:
                pl.when(chosen)(signal)
            else:
                signal()

    def meet(step):
        if step == 0:

            @pl.when(early < len(near))
            def _():
                pl.semaphore_wait(meet_sem.at[0], len(near) - early)

        else:
            pl.semaphore_wait(meet_sem.at[step], len(near))

    tell(0)

    def slot_block(d, s):
        return lax.rem(s + 2 * d, BLOCKS)

    def chunk_at(d, hops):
        return lax.rem(z + RING - hops, RING) if d == 0 else lax.rem(z + hops, RING)

    def z_copy(phase, d, s):
        ref = x.at[phase, chunk_at(d, lax.div(s, BLOCKS)), core, slot_block(d, s)]
        return pltpu.make_async_remote_copy(
            src_ref=ref,
            dst_ref=ref,
            send_sem=z_send.at[phase, d, s],
            recv_sem=z_recv.at[phase, d, s],
            device_id={"tp": up if d == 0 else down},
            device_id_type=MESH,
        )

    def z_arrival(phase, d, s):
        ref = x.at[phase, chunk_at(d, lax.div(s, BLOCKS) + 1), core, slot_block(d, s)]
        return pltpu.make_async_remote_copy(
            src_ref=ref,
            dst_ref=ref,
            send_sem=z_send.at[phase, d, s],
            recv_sem=z_recv.at[phase, d, s],
            device_id={"tp": up if d == 0 else down},
            device_id_type=MESH,
        )

    def d_copy(phase, index, chunk, b, half, count=2):
        ref = x.at[phase, chunk, half, pl.ds(b, count)]
        return pltpu.make_async_remote_copy(
            src_ref=ref,
            dst_ref=ref,
            send_sem=d_send.at[phase, index],
            recv_sem=d_recv.at[phase, index],
            device_id={"tp": partner},
            device_id_type=MESH,
        )

    def own_copy(phase, pair, half):
        return d_copy(phase, pair, z, 2 * pair, half)

    def pair_copy(phase, d, pair, half):
        s = 2 * pair
        chunk = chunk_at(d, lax.div(s, BLOCKS) + 1)
        return d_copy(phase, 2 + d * PAIRS + pair, chunk, slot_block(d, s), half)

    def slot_copy(phase, d, s, half):
        chunk = chunk_at(d, lax.div(s, BLOCKS) + 1)
        index = 2 + 2 * PAIRS + 2 * d + s - (SLOTS - 2)
        return d_copy(phase, index, chunk, slot_block(d, s), half, 1)

    def send_own(phase):
        for b in range(BLOCKS):
            z_copy(phase, 0, jnp.int32(b)).start()
            z_copy(phase, 1, jnp.int32(b)).start()
        for pair in range(2):
            own_copy(phase, pair, core).start()

    for copy in tok_copies:
        copy.wait()
    send_own(0)
    for copy in local_copies[1:]:
        copy.start()

    def id_copy(place, slot):
        return pltpu.make_async_remote_copy(
            src_ref=ids,
            dst_ref=ids_all.at[slot],
            send_sem=i_send.at[place],
            recv_sem=i_recv.at[place],
            device_id={"st": peer(place)},
            device_id_type=MESH,
        )

    def row_copy(place, slot):
        return pltpu.make_async_remote_copy(
            src_ref=outbox.at[place],
            dst_ref=inbox.at[slot],
            send_sem=s_send.at[place],
            recv_sem=s_recv.at[place],
            device_id={"st": peer(place)},
            device_id_type=MESH,
        )

    def wanted_row(read):
        wanted = jnp.int32(0)
        for pick in range(PICKS):
            for b in range(BLOCKS):
                ident = read(pick, b)
                mine = lax.shift_right_logical(ident, PASS_SHIFT) == st
                wanted = wanted + jnp.where(mine, ident & ((1 << PASS_SHIFT) - 1), 0)
        return wanted

    def send_ids(ring):
        for place in RINGS[ring]:
            id_copy(place, st).start()

    def gather_rows(ring):
        for place in RINGS[ring]:
            id_copy(place, source(place)).wait_recv()
        for place in RINGS[ring]:
            target = peer(place)
            outbox[place] = store_v[wanted_row(lambda pick, b: ids_all[target, pick, b])]

    def send_rows(ring):
        for place in RINGS[ring]:
            row_copy(place, st).start()

    def add_tokens(chunk, b, first=False):
        both = jnp.concatenate([x[0, chunk, 0, b], x[0, chunk, 1, b]], axis=1)
        rows = pl.ds(pl.multiple_of(chunk * 512, 512), 512)
        product = dot(both, wt[rows, :])
        wide = both.astype(F32)
        square = wide * wide
        gated = wide * wg_f[chunk]
        square = (square[:, 0:128] + square[:, 128:256]) + (
            square[:, 256:384] + square[:, 384:512]
        )
        gated = (gated[:, 0:128] + gated[:, 128:256]) + (gated[:, 256:384] + gated[:, 384:512])
        if first:
            acc[b] = product
            squares[b] = square
            gates[b] = gated
        else:
            acc[b] += product
            squares[b] += square
            gates[b] += gated

    def add_passages(chunk, b, first=False):
        both = jnp.concatenate([x[1, chunk, 0, b], x[1, chunk, 1, b]], axis=1)
        rows = pl.ds(pl.multiple_of(chunk * 512, 512), 512)
        product = dot(both, wm[rows, :])
        if first:
            acc_p[b] = product
        else:
            acc_p[b] += product

    def take_slot(phase, s, relay):
        for d in range(2):
            z_arrival(phase, d, s).wait_recv()
            if relay:
                z_copy(phase, d, s + BLOCKS).start()

    def add_one(phase, d, s):
        chunk = chunk_at(d, lax.div(s, BLOCKS) + 1)
        if phase == 0:
            add_tokens(chunk, slot_block(d, s))
        else:
            add_passages(chunk, slot_block(d, s))

    def hand_pair(phase, pair):
        for d in range(2):
            pair_copy(phase, d, pair, core).start()

    def add_pair(phase, pair):
        for d in range(2):
            pair_copy(phase, d, pair, other).wait_recv()
            add_one(phase, d, 2 * pair)
            add_one(phase, d, 2 * pair + 1)

    def hand_slot(phase, s):
        for d in range(2):
            slot_copy(phase, d, s, core).start()

    def add_slot(phase, s):
        for d in range(2):
            slot_copy(phase, d, s, other).wait_recv()
            add_one(phase, d, s)

    def add_own_tokens(pair):
        own_copy(0, pair, other).wait_recv()
        add_tokens(z, 2 * pair, first=True)
        add_tokens(z, 2 * pair + 1, first=True)

    def take(s):
        take_slot(0, jnp.int32(s), s < SLOTS - BLOCKS)
        if s % 2:
            hand_pair(0, jnp.int32(s // 2))

    def add(pair):
        add_pair(0, jnp.int32(pair))

    late = jnp.minimum(row, 2) + jnp.minimum(column, 2) >= 2
    soon = jnp.logical_not(late)

    def greet(ring):
        meet(ring)
        if ring + 1 < len(RINGS):
            tell(ring + 1)
        send_ids(ring)

    def gather_all():
        for ring in range(len(RINGS)):
            gather_rows(ring)

    def send_all():
        for ring in range(len(RINGS)):
            send_rows(ring)

    local_copies[0].wait()
    greet(0)

    @pl.when(late)
    def _():
        greet(1)
        greet(2)
        greet(3)

    take(0)

    @pl.when(soon)
    def _():
        greet(1)

    take(1)

    @pl.when(soon)
    def _():
        greet(2)

    local_copies[1].wait()
    inbox[st] = store_v[wanted_row(lambda pick, b: ids[pick, b])]
    take(2)

    @pl.when(soon)
    def _():
        greet(3)

    take(3)
    pl.when(late)(gather_all)
    take(4)
    pl.when(late)(send_all)
    take(5)
    pl.when(soon)(gather_all)
    for copy in local_copies[2:]:
        copy.wait()
    for chunk in range(RING):
        wg_f[chunk] = wg_v[:, chunk * 512 : (chunk + 1) * 512].astype(F32)
    add_own_tokens(0)
    take(6)
    pl.when(soon)(send_all)
    add_own_tokens(1)
    add(0)
    take(7)
    add(1)
    take(8)
    add(2)
    take(9)
    for place in range(N_ST - 1):
        row_copy(place, source(place)).wait_recv()
    for b in range(BLOCKS):
        for pick in range(PICKS):
            owner = lax.shift_right_logical(ids[pick, b], PASS_SHIFT)
            x[1, z, core, b, pick * PASS_ROWS : (pick + 1) * PASS_ROWS, :] = inbox[owner]

    add(3)
    send_own(1)
    take(10)
    add(4)
    take(11)
    take(12)
    add(5)
    take(13)

    rate = decay[0]

    def finish_tokens(b):
        mean_square = jnp.sum(squares[b], axis=1, keepdims=True) * (1.0 / D)
        scale = lax.rsqrt(mean_square + norm_eps)
        cosine = cos_v[b * BLOCK : (b + 1) * BLOCK, :]
        sine = sin_v[b * BLOCK : (b + 1) * BLOCK, :]

        def rotate(values):
            return values * cosine + pltpu.roll(values, KEY_DIM // 2, 1) * sine

        query = rotate(acc[b, :, 0:128] * scale).astype(BF16)
        key = (rotate(acc[b, :, 128:256] * scale) * KEY_DIM ** (-0.5)).astype(BF16)
        key_v[b * BLOCK : (b + 1) * BLOCK, :] = key
        value_v[b * BLOCK : (b + 1) * BLOCK, :] = (acc[b, :, 256:512] * scale).astype(BF16)
        memory = acc[b, :, 512:640]
        mean = jnp.mean(memory * memory, axis=1, keepdims=True)
        mem_q[b] = (memory * lax.rsqrt(mean + norm_eps)).astype(BF16)
        gate = jnp.sum(gates[b], axis=1, keepdims=True) * scale
        gate_v[b] = jnp.broadcast_to(jax.nn.sigmoid(gate), (BLOCK, 128))

        span = (b + 1) * BLOCK
        keys = key_v[0:span, :]
        values = value_v[0:span, :]
        row = lax.broadcasted_iota(jnp.int32, (BLOCK, span), 0) + b * BLOCK
        column = lax.broadcasted_iota(jnp.int32, (BLOCK, span), 1)
        distance = (row - column).astype(F32)
        mask = jnp.where(distance >= 0.0, jnp.exp(-rate * jnp.maximum(distance, 0.0)), 0.0)
        scores = dot_t(query, keys) * mask
        upper = scores.astype(BF16)
        lower = (scores - upper.astype(F32)).astype(BF16)
        mixed = dot(upper, values) + dot(lower, values)
        centred = mixed - jnp.mean(mixed, axis=1, keepdims=True)
        variance = jnp.mean(centred * centred, axis=1, keepdims=True)
        ret_norm[b] = centred * lax.rsqrt(variance + norm_eps)

    def finish_block(b):
        raw = acc_p[b, :, 0:128]
        mean = jnp.mean(raw * raw, axis=1, keepdims=True)
        pass_key = (raw * lax.rsqrt(mean + norm_eps)).astype(BF16)
        pass_value = acc_p[b, :, 128:256].astype(BF16)
        exponent = jnp.exp(dot_t(mem_q[b], pass_key) * MEM_DIM ** (-0.5))
        mass = jnp.sum(exponent, axis=1, keepdims=True)
        summed = dot(exponent.astype(BF16), pass_value)
        mem_out = (summed / mass).astype(BF16)
        lift = dot(mem_out, wl_v[0])
        gate = gate_v[b]
        gate = jnp.concatenate([gate, gate], axis=1)
        out[b * BLOCK : (b + 1) * BLOCK, :] = (ret_norm[b] + gate * lift).astype(BF16)

    for step in range(SLOTS):
        s = jnp.int32(step)
        take_slot(1, s, step < SLOTS - BLOCKS)
        if step >= SLOTS - 2:
            hand_slot(1, s)
        elif step % 2:
            hand_pair(1, jnp.int32(step // 2))
        if step == 0:
            add(PAIRS - 1)
            for pair in range(2):
                own_copy(1, pair, other).wait_recv()
                add_passages(z, 2 * pair, first=True)
                add_passages(z, 2 * pair + 1, first=True)
        elif step % 2 == 0:
            add_pair(1, jnp.int32(step // 2 - 1))
        if step < BLOCKS:
            finish_tokens(step)
        if step == 8:

            @pl.loop(0, SLOTS)
            def _(n):
                z_copy(0, 0, n).wait_send()
                z_copy(0, 1, n).wait_send()

            @pl.loop(0, 2 + 2 * PAIRS)
            def _(n):
                d_copy(0, n, z, 0, core).wait_send()

            for place in range(N_ST - 1):
                id_copy(place, st).wait_send()
                row_copy(place, st).wait_send()

    add_slot(1, jnp.int32(SLOTS - 2))
    finish_block(0)
    finish_block(2)
    add_slot(1, jnp.int32(SLOTS - 1))
    finish_block(1)
    finish_block(3)

    @pl.loop(0, SLOTS)
    def _(n):
        z_copy(1, 0, n).wait_send()
        z_copy(1, 1, n).wait_send()

    for pair in range(2):
        own_copy(1, pair, core).wait_send()
    for pair in range(PAIRS - 1):
        for d in range(2):
            pair_copy(1, d, pair, core).wait_send()
    for s in (SLOTS - 2, SLOTS - 1):
        for d in range(2):
            slot_copy(1, d, s, core).wait_send()


def per_device(
    tokens,
    w_query,
    w_key,
    w_value,
    w_mem_query,
    w_mem_key,
    w_mem_value,
    w_gate,
    w_lift,
    decay_rate,
    store,
    passage_ids,
):
    cos_table, sin_table = rotary_tables()
    hbm = pl.BlockSpec(memory_space=pltpu.HBM)
    dma = pltpu.SemaphoreType.DMA
    operands = (
        tokens,
        w_query,
        w_key,
        w_value,
        w_mem_query,
        w_mem_key,
        w_mem_value,
        w_gate.reshape(1, D),
        w_lift,
        store,
        jnp.asarray(cos_table),
        jnp.asarray(sin_table),
        passage_ids.T,
    )
    return pl.pallas_call(
        kernel,
        out_shape=pltpu.VMEM((SEQ_LEN, VALUE_DIM), BF16),
        in_specs=[pl.BlockSpec(memory_space=pltpu.SMEM)] + [hbm] * 13,
        out_specs=pl.BlockSpec(memory_space=pltpu.VMEM),
        scratch_shapes=[
            pltpu.VMEM((2, RING, 2, BLOCKS, BLOCK, HALF), BF16),
            pltpu.VMEM((D, TOK_COLS), BF16),
            pltpu.VMEM((D, 2 * MEM_DIM), BF16),
            pltpu.VMEM(store.shape, BF16),
            pltpu.VMEM((N_ST, PASS_ROWS, HALF), BF16),
            pltpu.VMEM((N_ST, PASS_ROWS, HALF), BF16),
            pltpu.VMEM((BLOCKS, BLOCK, TOK_COLS), F32),
            pltpu.VMEM((BLOCKS, BLOCK, 128), F32),
            pltpu.VMEM((BLOCKS, BLOCK, 128), F32),
            pltpu.VMEM((BLOCKS, BLOCK, 2 * MEM_DIM), F32),
            pltpu.VMEM((SEQ_LEN, KEY_DIM), BF16),
            pltpu.VMEM((SEQ_LEN, VALUE_DIM), BF16),
            pltpu.VMEM((BLOCKS, BLOCK, MEM_DIM), BF16),
            pltpu.VMEM((BLOCKS, BLOCK, 128), F32),
            pltpu.VMEM((BLOCKS, BLOCK, VALUE_DIM), F32),
            pltpu.VMEM((1, D), BF16),
            pltpu.VMEM((RING, 1, 512), F32),
            pltpu.VMEM((1, MEM_DIM, VALUE_DIM), BF16),
            pltpu.VMEM((SEQ_LEN, KEY_DIM), F32),
            pltpu.VMEM((SEQ_LEN, KEY_DIM), F32),
            pltpu.SMEM((PICKS, BLOCKS), jnp.int32),
            pltpu.SMEM((N_ST, PICKS, BLOCKS), jnp.int32),
            dma((BLOCKS,)),
            dma((12,)),
            dma((2, 2, SLOTS)),
            dma((2, 2, SLOTS)),
            dma((2, 6 + 2 * PAIRS)),
            dma((2, 6 + 2 * PAIRS)),
            dma((N_ST,)),
            dma((N_ST,)),
            dma((N_ST,)),
            dma((N_ST,)),
            pltpu.SemaphoreType.REGULAR((4,)),
        ],
        compiler_params=pltpu.CompilerParams(
            collective_id=0, has_side_effects=True, vmem_limit_bytes=48 * 1024 * 1024
        ),
        name="fused_layer",
    )(decay_rate, *[pltpu.with_memory_space_constraint(array, pltpu.HBM) for array in operands])


def solution(mesh):
    in_specs = (
        P("st", "tp"),
        P(None, "tp"),
        P(None, "tp"),
        P(None, "tp"),
        P(None, "tp"),
        P(None, "tp"),
        P(None, "tp"),
        P(None, "tp"),
        P("tp", None, None),
        P("tp"),
        P("st", None, "tp"),
        P("st", None),
    )
    out_specs = P("st", "tp")
    return jax.shard_map(
        per_device, mesh=mesh, in_specs=in_specs, out_specs=out_specs, check_vma=False
    )
```

```python
import jax
import jax.numpy as jnp
import numpy as np
from jax import lax
from jax.experimental import pallas as pl
from jax.experimental.pallas import tpu as pltpu
from jax.sharding import PartitionSpec as P

D = 4096
KEY_DIM = 128
VALUE_DIM = 256
MEM_DIM = 128
SEQ_LEN = 512
BLOCK = 128
PICKS = 2
PASS_ROWS = 64
PASS_SHIFT = 7
N_ST = 16
RING = 8
BLOCKS = 4
SLOTS = 14
HALF = 256
TOK_COLS = 640

STEPS = sorted(
    ((a, b) for a in range(4) for b in range(4) if a or b),
    key=lambda step: sum(min(part, 4 - part) for part in step),
)
RINGS = [range(0, 4), range(4, 10), range(10, 14), range(14, 15)]

norm_eps = 1e-06
rope_base = 10000.0

F32 = jnp.float32
BF16 = jnp.bfloat16
MESH = pl.DeviceIdType.MESH


def rotary_tables():
    half = KEY_DIM // 2
    inverse = rope_base ** (-np.arange(half, dtype=np.float64) / half)
    angles = np.arange(SEQ_LEN, dtype=np.float64)[:, None] * inverse[None, :]
    cosine, sine = np.cos(angles), np.sin(angles)
    cos_table = np.concatenate([cosine, cosine], axis=1).astype(np.float32)
    sin_table = np.concatenate([-sine, sine], axis=1).astype(np.float32)
    return cos_table, sin_table


def dot(a, b):
    return jnp.dot(a, b, preferred_element_type=F32)


def dot_t(a, b):
    return lax.dot_general(a, b, (((1,), (1,)), ((), ())), preferred_element_type=F32)


def kernel(
    decay,
    tok,
    wq,
    wk,
    wv,
    wmq,
    wmk,
    wmv,
    wg,
    wl,
    store,
    cos_in,
    sin_in,
    ids_in,
    out,
    x,
    wt,
    wm,
    store_v,
    outbox,
    inbox,
    acc,
    squares,
    gates,
    acc_p,
    key_v,
    value_v,
    mem_q,
    gate_v,
    ret_norm,
    wg_v,
    wg_f,
    wl_v,
    cos_v,
    sin_v,
    ids,
    ids_all,
    tok_sem,
    local_sem,
    z_send,
    z_recv,
    d_send,
    d_recv,
    i_send,
    i_recv,
    s_send,
    s_recv,
    meet_sem,
):
    st = lax.axis_index("st")
    tp = lax.axis_index("tp")
    z = lax.div(tp, 2)
    core = lax.rem(tp, 2)
    other = 1 - core
    up = lax.rem(z + 1, RING) * 2 + core
    down = lax.rem(z + RING - 1, RING) * 2 + core
    partner = z * 2 + other

    side = 4
    row, column = lax.div(st, side), lax.rem(st, side)

    def peer(place):
        down_by, right_by = STEPS[place]
        return lax.rem(row + down_by, side) * side + lax.rem(column + right_by, side)

    def source(place):
        down_by, right_by = STEPS[place]
        return lax.rem(row + side - down_by, side) * side + lax.rem(
            column + side - right_by, side
        )

    near = (
        lax.rem(row + 1, side) * side + column,
        lax.rem(row + side - 1, side) * side + column,
        row * side + lax.rem(column + 1, side),
        row * side + lax.rem(column + side - 1, side),
    )

    tok_copies = [
        pltpu.make_async_copy(
            tok.at[pl.ds(b * BLOCK, BLOCK), :], x.at[0, z, core, b], tok_sem.at[b]
        )
        for b in range(BLOCKS)
    ]
    for copy in tok_copies:
        copy.start()
    local = [
        (ids_in, ids),
        (store, store_v),
        (wg, wg_v),
        (wq, wt.at[:, pl.ds(0, 128)]),
        (wk, wt.at[:, pl.ds(128, 128)]),
        (wv, wt.at[:, pl.ds(256, 256)]),
        (wmq, wt.at[:, pl.ds(512, 128)]),
        (wmk, wm.at[:, pl.ds(0, 128)]),
        (wmv, wm.at[:, pl.ds(128, 128)]),
        (wl, wl_v),
        (cos_in, cos_v),
        (sin_in, sin_v),
    ]
    local_copies = [
        pltpu.make_async_copy(src, dst, local_sem.at[i]) for i, (src, dst) in enumerate(local)
    ]
    local_copies[0].start()

    barrier = pltpu.get_barrier_semaphore()
    for target in (up, down, partner):
        pl.semaphore_signal(barrier, inc=1, device_id={"tp": target}, device_id_type=MESH)
    ahead = (row < side - 1, row == 0, column < side - 1, column == 0)
    behind = (row == side - 1, row > 0, column == side - 1, column > 0)
    for target, chosen in zip(near, ahead):

        @pl.when(chosen)
        def _():
            pl.semaphore_signal(barrier, inc=1, device_id={"st": target}, device_id_type=MESH)

    early = sum(one.astype(jnp.int32) for one in behind)
    pl.semaphore_wait(barrier, 3 + early)

    def tell(step):
        for target, chosen in zip(near, behind):

            def signal():
                pl.semaphore_signal(
                    meet_sem.at[step], inc=1, device_id={"st": target}, device_id_type=MESH
                )

            if step == 0:
                pl.when(chosen)(signal)
            else:
                signal()

    def meet(step):
        if step == 0:

            @pl.when(early < len(near))
            def _():
                pl.semaphore_wait(meet_sem.at[0], len(near) - early)

        else:
            pl.semaphore_wait(meet_sem.at[step], len(near))

    tell(0)

    def slot_block(d, s):
        return lax.rem(s + 2 * d, BLOCKS)

    def chunk_at(d, hops):
        return lax.rem(z + RING - hops, RING) if d == 0 else lax.rem(z + hops, RING)

    def z_copy(phase, d, s):
        ref = x.at[phase, chunk_at(d, lax.div(s, BLOCKS)), core, slot_block(d, s)]
        return pltpu.make_async_remote_copy(
            src_ref=ref,
            dst_ref=ref,
            send_sem=z_send.at[phase, d, s],
            recv_sem=z_recv.at[phase, d, s],
            device_id={"tp": up if d == 0 else down},
            device_id_type=MESH,
        )

    def z_arrival(phase, d, s):
        ref = x.at[phase, chunk_at(d, lax.div(s, BLOCKS) + 1), core, slot_block(d, s)]
        return pltpu.make_async_remote_copy(
            src_ref=ref,
            dst_ref=ref,
            send_sem=z_send.at[phase, d, s],
            recv_sem=z_recv.at[phase, d, s],
            device_id={"tp": up if d == 0 else down},
            device_id_type=MESH,
        )

    def hand_copy(phase, d, s, half, count):
        chunk = chunk_at(d, s // BLOCKS + 1)
        ref = x.at[phase, chunk, half, pl.ds((s + 2 * d) % BLOCKS, count)] if count < BLOCKS else x.at[phase, chunk, half]
        index = BLOCKS + s
        return pltpu.make_async_remote_copy(
            src_ref=ref,
            dst_ref=ref,
            send_sem=d_send.at[phase, d, index],
            recv_sem=d_recv.at[phase, d, index],
            device_id={"tp": partner},
            device_id_type=MESH,
        )

    def send_own(phase):
        for b in range(BLOCKS):
            z_copy(phase, 0, jnp.int32(b)).start()
            z_copy(phase, 1, jnp.int32(b)).start()
        hand_copy(phase, 0, -BLOCKS, core, BLOCKS).start()

    for copy in tok_copies:
        copy.wait()
    send_own(0)
    for copy in local_copies[1:]:
        copy.start()

    def id_copy(place, slot):
        return pltpu.make_async_remote_copy(
            src_ref=ids,
            dst_ref=ids_all.at[slot],
            send_sem=i_send.at[place],
            recv_sem=i_recv.at[place],
            device_id={"st": peer(place)},
            device_id_type=MESH,
        )

    def row_copy(place, slot):
        return pltpu.make_async_remote_copy(
            src_ref=outbox.at[place],
            dst_ref=inbox.at[slot],
            send_sem=s_send.at[place],
            recv_sem=s_recv.at[place],
            device_id={"st": peer(place)},
            device_id_type=MESH,
        )

    def wanted_row(read):
        wanted = jnp.int32(0)
        for pick in range(PICKS):
            for b in range(BLOCKS):
                ident = read(pick, b)
                mine = lax.shift_right_logical(ident, PASS_SHIFT) == st
                wanted = wanted + jnp.where(mine, ident & ((1 << PASS_SHIFT) - 1), 0)
        return wanted

    def send_ids(ring):
        for place in RINGS[ring]:
            id_copy(place, st).start()

    def gather_rows(ring):
        for place in RINGS[ring]:
            id_copy(place, source(place)).wait_recv()
        for place in RINGS[ring]:
            target = peer(place)
            outbox[place] = store_v[wanted_row(lambda pick, b: ids_all[target, pick, b])]

    def send_rows(ring):
        for place in RINGS[ring]:
            row_copy(place, st).start()

    def add_tokens(chunk, b, first=False):
        both = jnp.concatenate([x[0, chunk, 0, b], x[0, chunk, 1, b]], axis=1)
        rows = pl.ds(pl.multiple_of(chunk * 512, 512), 512)
        product = dot(both, wt[rows, :])
        wide = both.astype(F32)
        square = wide * wide
        gated = wide * wg_f[chunk]
        square = (square[:, 0:128] + square[:, 128:256]) + (
            square[:, 256:384] + square[:, 384:512]
        )
        gated = (gated[:, 0:128] + gated[:, 128:256]) + (gated[:, 256:384] + gated[:, 384:512])
        if first:
            acc[b] = product
            squares[b] = square
            gates[b] = gated
        else:
            acc[b] += product
            squares[b] += square
            gates[b] += gated

    def add_passages(chunk, b, first=False):
        both = jnp.concatenate([x[1, chunk, 0, b], x[1, chunk, 1, b]], axis=1)
        rows = pl.ds(pl.multiple_of(chunk * 512, 512), 512)
        product = dot(both, wm[rows, :])
        if first:
            acc_p[b] = product
        else:
            acc_p[b] += product

    def take_slot(phase, s, relay):
        for d in range(2):
            z_arrival(phase, d, s).wait_recv()
            if relay:
                z_copy(phase, d, s + BLOCKS).start()

    def add_one(phase, d, s):
        chunk = chunk_at(d, lax.div(s, BLOCKS) + 1)
        if phase == 0:
            add_tokens(chunk, slot_block(d, s))
        else:
            add_passages(chunk, slot_block(d, s))

    hand_groups = (
        ((0, 2), (2, 2), (4, 2), (6, 2), (8, 2), (10, 2), (12, 2)),
        ((0, 2), (2, 2), (4, 2), (6, 2), (8, 2), (10, 2), (12, 1), (13, 1)),
    )

    def take(phase, s):
        take_slot(phase, jnp.int32(s), s < SLOTS - BLOCKS)
        for first, count in hand_groups[phase]:
            if s == first + count - 1:
                for d in range(2):
                    hand_copy(phase, d, first, core, count).start()

    def add(phase, *slots):
        for s in slots:
            for d in range(2):
                for first, count in hand_groups[phase]:
                    if s == first:
                        hand_copy(phase, d, first, other, count).wait_recv()
                add_one(phase, d, jnp.int32(s))

    def add_own(phase):
        hand_copy(phase, 0, -BLOCKS, other, BLOCKS).wait_recv()
        for b in range(BLOCKS):
            if phase == 0:
                add_tokens(z, b, first=True)
            else:
                add_passages(z, b, first=True)

    late = jnp.minimum(row, 2) + jnp.minimum(column, 2) >= 2
    soon = jnp.logical_not(late)

    def greet(ring):
        meet(ring)
        if ring + 1 < len(RINGS):
            tell(ring + 1)
        send_ids(ring)

    def gather_all():
        for ring in range(len(RINGS)):
            gather_rows(ring)

    def send_all():
        for ring in range(len(RINGS)):
            send_rows(ring)

    local_copies[0].wait()
    greet(0)

    @pl.when(late)
    def _():
        greet(1)
        greet(2)
        greet(3)

    take(0, 0)

    @pl.when(soon)
    def _():
        greet(1)

    take(0, 1)

    @pl.when(soon)
    def _():
        greet(2)

    local_copies[1].wait()
    inbox[st] = store_v[wanted_row(lambda pick, b: ids[pick, b])]
    take(0, 2)

    @pl.when(soon)
    def _():
        greet(3)

    take(0, 3)
    pl.when(late)(gather_all)
    take(0, 4)
    pl.when(late)(send_all)
    take(0, 5)
    pl.when(soon)(gather_all)
    for copy in local_copies[2:]:
        copy.wait()
    for chunk in range(RING):
        wg_f[chunk] = wg_v[:, chunk * 512 : (chunk + 1) * 512].astype(F32)
    add_own(0)
    take(0, 6)
    pl.when(soon)(send_all)
    add(0, 0, 1)
    take(0, 7)
    add(0, 2, 3)
    take(0, 8)
    add(0, 4, 5)
    take(0, 9)
    for place in range(N_ST - 1):
        row_copy(place, source(place)).wait_recv()
    for b in range(BLOCKS):
        for pick in range(PICKS):
            owner = lax.shift_right_logical(ids[pick, b], PASS_SHIFT)
            x[1, z, core, b, pick * PASS_ROWS : (pick + 1) * PASS_ROWS, :] = inbox[owner]

    add(0, 6)
    send_own(1)
    add(0, 7)
    take(0, 10)
    take(0, 11)
    take(0, 12)
    add(0, 8, 9)
    take(0, 13)
    add(0, 10, 11)

    rate = decay[0]

    def finish_tokens(b):
        mean_square = jnp.sum(squares[b], axis=1, keepdims=True) * (1.0 / D)
        scale = lax.rsqrt(mean_square + norm_eps)
        cosine = cos_v[b * BLOCK : (b + 1) * BLOCK, :]
        sine = sin_v[b * BLOCK : (b + 1) * BLOCK, :]

        def rotate(values):
            return values * cosine + pltpu.roll(values, KEY_DIM // 2, 1) * sine

        query = rotate(acc[b, :, 0:128] * scale).astype(BF16)
        key = (rotate(acc[b, :, 128:256] * scale) * KEY_DIM ** (-0.5)).astype(BF16)
        key_v[b * BLOCK : (b + 1) * BLOCK, :] = key
        value_v[b * BLOCK : (b + 1) * BLOCK, :] = (acc[b, :, 256:512] * scale).astype(BF16)
        memory = acc[b, :, 512:640]
        mean = jnp.mean(memory * memory, axis=1, keepdims=True)
        mem_q[b] = (memory * lax.rsqrt(mean + norm_eps)).astype(BF16)
        gate = jnp.sum(gates[b], axis=1, keepdims=True) * scale
        gate_v[b] = jnp.broadcast_to(jax.nn.sigmoid(gate), (BLOCK, 128))

        span = (b + 1) * BLOCK
        keys = key_v[0:span, :]
        values = value_v[0:span, :]
        row = lax.broadcasted_iota(jnp.int32, (BLOCK, span), 0) + b * BLOCK
        column = lax.broadcasted_iota(jnp.int32, (BLOCK, span), 1)
        distance = (row - column).astype(F32)
        mask = jnp.where(distance >= 0.0, jnp.exp(-rate * jnp.maximum(distance, 0.0)), 0.0)
        scores = dot_t(query, keys) * mask
        upper = scores.astype(BF16)
        lower = (scores - upper.astype(F32)).astype(BF16)
        mixed = dot(upper, values) + dot(lower, values)
        centred = mixed - jnp.mean(mixed, axis=1, keepdims=True)
        variance = jnp.mean(centred * centred, axis=1, keepdims=True)
        ret_norm[b] = centred * lax.rsqrt(variance + norm_eps)

    def finish_block(b):
        raw = acc_p[b, :, 0:128]
        mean = jnp.mean(raw * raw, axis=1, keepdims=True)
        pass_key = (raw * lax.rsqrt(mean + norm_eps)).astype(BF16)
        lifted = dot(acc_p[b, :, 128:256].astype(BF16), wl_v[0]).astype(BF16)
        exponent = jnp.exp(dot_t(mem_q[b], pass_key) * MEM_DIM ** (-0.5))
        mass = jnp.sum(exponent, axis=1, keepdims=True)
        gate = gate_v[b] / mass
        gate = jnp.concatenate([gate, gate], axis=1)
        lift = dot(exponent.astype(BF16), lifted)
        out[b * BLOCK : (b + 1) * BLOCK, :] = (ret_norm[b] + gate * lift).astype(BF16)

    def hand_done(phase):
        hand_copy(phase, 0, -BLOCKS, core, BLOCKS).wait_send()
        for d in range(2):
            for first, count in hand_groups[phase]:
                hand_copy(phase, d, first, core, count).wait_send()

    for step in range(SLOTS):
        take(1, step)
        if step == 0:
            add(0, 12, 13)
            add_own(1)
        if step % 2 == 0 and step > 0:
            add(1, step - 2, step - 1)
        if 1 <= step <= BLOCKS:
            finish_tokens(step - 1)
        if step == 9:

            @pl.loop(0, SLOTS)
            def _(n):
                z_copy(0, 0, n).wait_send()
                z_copy(0, 1, n).wait_send()

            hand_done(0)
            for place in range(N_ST - 1):
                id_copy(place, st).wait_send()
                row_copy(place, st).wait_send()

    add(1, 12)
    finish_block(0)
    finish_block(2)
    add(1, 13)
    finish_block(1)
    finish_block(3)

    @pl.loop(0, SLOTS)
    def _(n):
        z_copy(1, 0, n).wait_send()
        z_copy(1, 1, n).wait_send()

    hand_done(1)


def per_device(
    tokens,
    w_query,
    w_key,
    w_value,
    w_mem_query,
    w_mem_key,
    w_mem_value,
    w_gate,
    w_lift,
    decay_rate,
    store,
    passage_ids,
):
    cos_table, sin_table = rotary_tables()
    hbm = pl.BlockSpec(memory_space=pltpu.HBM)
    dma = pltpu.SemaphoreType.DMA
    operands = (
        tokens,
        w_query,
        w_key,
        w_value,
        w_mem_query,
        w_mem_key,
        w_mem_value,
        w_gate.reshape(1, D),
        w_lift,
        store,
        jnp.asarray(cos_table),
        jnp.asarray(sin_table),
        passage_ids.T,
    )
    return pl.pallas_call(
        kernel,
        out_shape=pltpu.VMEM((SEQ_LEN, VALUE_DIM), BF16),
        in_specs=[pl.BlockSpec(memory_space=pltpu.SMEM)] + [hbm] * 13,
        out_specs=pl.BlockSpec(memory_space=pltpu.VMEM),
        scratch_shapes=[
            pltpu.VMEM((2, RING, 2, BLOCKS, BLOCK, HALF), BF16),
            pltpu.VMEM((D, TOK_COLS), BF16),
            pltpu.VMEM((D, 2 * MEM_DIM), BF16),
            pltpu.VMEM(store.shape, BF16),
            pltpu.VMEM((N_ST, PASS_ROWS, HALF), BF16),
            pltpu.VMEM((N_ST, PASS_ROWS, HALF), BF16),
            pltpu.VMEM((BLOCKS, BLOCK, TOK_COLS), F32),
            pltpu.VMEM((BLOCKS, BLOCK, 128), F32),
            pltpu.VMEM((BLOCKS, BLOCK, 128), F32),
            pltpu.VMEM((BLOCKS, BLOCK, 2 * MEM_DIM), F32),
            pltpu.VMEM((SEQ_LEN, KEY_DIM), BF16),
            pltpu.VMEM((SEQ_LEN, VALUE_DIM), BF16),
            pltpu.VMEM((BLOCKS, BLOCK, MEM_DIM), BF16),
            pltpu.VMEM((BLOCKS, BLOCK, 128), F32),
            pltpu.VMEM((BLOCKS, BLOCK, VALUE_DIM), F32),
            pltpu.VMEM((1, D), BF16),
            pltpu.VMEM((RING, 1, 512), F32),
            pltpu.VMEM((1, MEM_DIM, VALUE_DIM), BF16),
            pltpu.VMEM((SEQ_LEN, KEY_DIM), F32),
            pltpu.VMEM((SEQ_LEN, KEY_DIM), F32),
            pltpu.SMEM((PICKS, BLOCKS), jnp.int32),
            pltpu.SMEM((N_ST, PICKS, BLOCKS), jnp.int32),
            dma((BLOCKS,)),
            dma((12,)),
            dma((2, 2, SLOTS)),
            dma((2, 2, SLOTS)),
            dma((2, 2, BLOCKS + SLOTS)),
            dma((2, 2, BLOCKS + SLOTS)),
            dma((N_ST,)),
            dma((N_ST,)),
            dma((N_ST,)),
            dma((N_ST,)),
            pltpu.SemaphoreType.REGULAR((4,)),
        ],
        compiler_params=pltpu.CompilerParams(
            collective_id=0, has_side_effects=True, vmem_limit_bytes=48 * 1024 * 1024
        ),
        name="fused_layer",
    )(decay_rate, *[pltpu.with_memory_space_constraint(array, pltpu.HBM) for array in operands])


def solution(mesh):
    in_specs = (
        P("st", "tp"),
        P(None, "tp"),
        P(None, "tp"),
        P(None, "tp"),
        P(None, "tp"),
        P(None, "tp"),
        P(None, "tp"),
        P(None, "tp"),
        P("tp", None, None),
        P("tp"),
        P("st", None, "tp"),
        P("st", None),
    )
    out_specs = P("st", "tp")
    return jax.shard_map(
        per_device, mesh=mesh, in_specs=in_specs, out_specs=out_specs, check_vma=False
    )
```

```python
import jax
import jax.numpy as jnp
import numpy as np
from jax import lax
from jax.experimental import pallas as pl
from jax.experimental.pallas import tpu as pltpu
from jax.sharding import PartitionSpec as P

D = 4096
KEY_DIM = 128
VALUE_DIM = 256
MEM_DIM = 128
SEQ_LEN = 512
BLOCK = 128
PICKS = 2
PASS_ROWS = 64
PASS_SHIFT = 7
N_ST = 16
RING = 8
BLOCKS = 4
SLOTS = 14
HALF = 256
TOK_COLS = 640

STEPS = sorted(
    ((a, b) for a in range(4) for b in range(4) if a or b),
    key=lambda step: sum(min(part, 4 - part) for part in step),
)
RINGS = [range(0, 4), range(4, 10), range(10, 14), range(14, 15)]

norm_eps = 1e-06
rope_base = 10000.0

F32 = jnp.float32
BF16 = jnp.bfloat16
MESH = pl.DeviceIdType.MESH


def rotary_tables():
    half = KEY_DIM // 2
    inverse = rope_base ** (-np.arange(half, dtype=np.float64) / half)
    angles = np.arange(SEQ_LEN, dtype=np.float64)[:, None] * inverse[None, :]
    cosine, sine = np.cos(angles), np.sin(angles)
    cos_table = np.concatenate([cosine, cosine], axis=1).astype(np.float32)
    sin_table = np.concatenate([-sine, sine], axis=1).astype(np.float32)
    return cos_table, sin_table


def dot(a, b):
    return jnp.dot(a, b, preferred_element_type=F32)


def dot_t(a, b):
    return lax.dot_general(a, b, (((1,), (1,)), ((), ())), preferred_element_type=F32)


def kernel(
    decay,
    tok,
    wq,
    wk,
    wv,
    wmq,
    wmk,
    wmv,
    wg,
    wl,
    store,
    cos_in,
    sin_in,
    ids_in,
    out,
    x,
    wt,
    wm,
    store_v,
    outbox,
    inbox,
    acc,
    squares,
    gates,
    acc_p,
    key_v,
    value_v,
    mem_q,
    gate_v,
    ret_norm,
    wg_v,
    wg_f,
    wl_v,
    cos_v,
    sin_v,
    ids,
    ids_all,
    tok_sem,
    local_sem,
    z_send,
    z_recv,
    d_send,
    d_recv,
    i_send,
    i_recv,
    s_send,
    s_recv,
    meet_sem,
):
    st = lax.axis_index("st")
    tp = lax.axis_index("tp")
    z = lax.div(tp, 2)
    core = lax.rem(tp, 2)
    other = 1 - core
    up = lax.rem(z + 1, RING) * 2 + core
    down = lax.rem(z + RING - 1, RING) * 2 + core
    partner = z * 2 + other

    side = 4
    row, column = lax.div(st, side), lax.rem(st, side)

    def peer(place):
        down_by, right_by = STEPS[place]
        return lax.rem(row + down_by, side) * side + lax.rem(column + right_by, side)

    def source(place):
        down_by, right_by = STEPS[place]
        return lax.rem(row + side - down_by, side) * side + lax.rem(
            column + side - right_by, side
        )

    near = (
        lax.rem(row + 1, side) * side + column,
        lax.rem(row + side - 1, side) * side + column,
        row * side + lax.rem(column + 1, side),
        row * side + lax.rem(column + side - 1, side),
    )

    tok_copies = [
        pltpu.make_async_copy(
            tok.at[pl.ds(b * BLOCK, BLOCK), :], x.at[0, z, core, b], tok_sem.at[b]
        )
        for b in range(BLOCKS)
    ]
    for copy in tok_copies:
        copy.start()
    local = [
        (ids_in, ids),
        (store, store_v),
        (wg, wg_v),
        (wq, wt.at[:, pl.ds(0, 128)]),
        (wk, wt.at[:, pl.ds(128, 128)]),
        (wv, wt.at[:, pl.ds(256, 256)]),
        (wmq, wt.at[:, pl.ds(512, 128)]),
        (wmk, wm.at[:, pl.ds(0, 128)]),
        (wmv, wm.at[:, pl.ds(128, 128)]),
        (wl, wl_v),
        (cos_in, cos_v),
        (sin_in, sin_v),
    ]
    local_copies = [
        pltpu.make_async_copy(src, dst, local_sem.at[i]) for i, (src, dst) in enumerate(local)
    ]
    local_copies[0].start()

    barrier = pltpu.get_barrier_semaphore()
    for target in (up, down, partner):
        pl.semaphore_signal(barrier, inc=1, device_id={"tp": target}, device_id_type=MESH)
    ahead = (row < side - 1, row == 0, column < side - 1, column == 0)
    behind = (row == side - 1, row > 0, column == side - 1, column > 0)
    for target, chosen in zip(near, ahead):

        @pl.when(chosen)
        def _():
            pl.semaphore_signal(barrier, inc=1, device_id={"st": target}, device_id_type=MESH)

    early = sum(one.astype(jnp.int32) for one in behind)
    pl.semaphore_wait(barrier, 3 + early)

    def tell(step):
        for target, chosen in zip(near, behind):

            def signal():
                pl.semaphore_signal(
                    meet_sem.at[step], inc=1, device_id={"st": target}, device_id_type=MESH
                )

            if step == 0:
                pl.when(chosen)(signal)
            else:
                signal()

    def meet(step):
        if step == 0:

            @pl.when(early < len(near))
            def _():
                pl.semaphore_wait(meet_sem.at[0], len(near) - early)

        else:
            pl.semaphore_wait(meet_sem.at[step], len(near))

    tell(0)

    def slot_block(d, s):
        return lax.rem(s + 2 * d, BLOCKS)

    def chunk_at(d, hops):
        return lax.rem(z + RING - hops, RING) if d == 0 else lax.rem(z + hops, RING)

    def z_copy(phase, d, s):
        ref = x.at[phase, chunk_at(d, lax.div(s, BLOCKS)), core, slot_block(d, s)]
        return pltpu.make_async_remote_copy(
            src_ref=ref,
            dst_ref=ref,
            send_sem=z_send.at[phase, d, s],
            recv_sem=z_recv.at[phase, d, s],
            device_id={"tp": up if d == 0 else down},
            device_id_type=MESH,
        )

    def z_arrival(phase, d, s):
        ref = x.at[phase, chunk_at(d, lax.div(s, BLOCKS) + 1), core, slot_block(d, s)]
        return pltpu.make_async_remote_copy(
            src_ref=ref,
            dst_ref=ref,
            send_sem=z_send.at[phase, d, s],
            recv_sem=z_recv.at[phase, d, s],
            device_id={"tp": up if d == 0 else down},
            device_id_type=MESH,
        )

    def hand_copy(phase, d, s, half, count):
        chunk = chunk_at(d, s // BLOCKS + 1)
        ref = x.at[phase, chunk, half, pl.ds((s + 2 * d) % BLOCKS, count)] if count < BLOCKS else x.at[phase, chunk, half]
        index = BLOCKS + s
        return pltpu.make_async_remote_copy(
            src_ref=ref,
            dst_ref=ref,
            send_sem=d_send.at[phase, d, index],
            recv_sem=d_recv.at[phase, d, index],
            device_id={"tp": partner},
            device_id_type=MESH,
        )

    def send_own(phase):
        for b in range(BLOCKS):
            z_copy(phase, 0, jnp.int32(b)).start()
            z_copy(phase, 1, jnp.int32(b)).start()
        hand_copy(phase, 0, -BLOCKS, core, BLOCKS).start()

    for copy in tok_copies:
        copy.wait()
    send_own(0)
    for copy in local_copies[1:]:
        copy.start()

    def id_copy(place, slot):
        return pltpu.make_async_remote_copy(
            src_ref=ids,
            dst_ref=ids_all.at[slot],
            send_sem=i_send.at[place],
            recv_sem=i_recv.at[place],
            device_id={"st": peer(place)},
            device_id_type=MESH,
        )

    def row_copy(place, slot):
        return pltpu.make_async_remote_copy(
            src_ref=outbox.at[place],
            dst_ref=inbox.at[slot],
            send_sem=s_send.at[place],
            recv_sem=s_recv.at[place],
            device_id={"st": peer(place)},
            device_id_type=MESH,
        )

    def wanted_row(read):
        wanted = jnp.int32(0)
        for pick in range(PICKS):
            for b in range(BLOCKS):
                ident = read(pick, b)
                mine = lax.shift_right_logical(ident, PASS_SHIFT) == st
                wanted = wanted + jnp.where(mine, ident & ((1 << PASS_SHIFT) - 1), 0)
        return wanted

    def send_ids(ring):
        for place in RINGS[ring]:
            id_copy(place, st).start()

    def gather_rows(ring):
        for place in RINGS[ring]:
            id_copy(place, source(place)).wait_recv()
        for place in RINGS[ring]:
            target = peer(place)
            outbox[place] = store_v[wanted_row(lambda pick, b: ids_all[target, pick, b])]

    def send_rows(ring):
        for place in RINGS[ring]:
            row_copy(place, st).start()

    def add_tokens(chunk, b, first=False):
        both = jnp.concatenate([x[0, chunk, 0, b], x[0, chunk, 1, b]], axis=1)
        rows = pl.ds(pl.multiple_of(chunk * 512, 512), 512)
        product = dot(both, wt[rows, :])
        wide = both.astype(F32)
        square = wide * wide
        gated = wide * wg_f[chunk]
        square = (square[:, 0:128] + square[:, 128:256]) + (
            square[:, 256:384] + square[:, 384:512]
        )
        gated = (gated[:, 0:128] + gated[:, 128:256]) + (gated[:, 256:384] + gated[:, 384:512])
        if first:
            acc[b] = product
            squares[b] = square
            gates[b] = gated
        else:
            acc[b] += product
            squares[b] += square
            gates[b] += gated

    def add_passages(chunk, b, first=False):
        both = jnp.concatenate([x[1, chunk, 0, b], x[1, chunk, 1, b]], axis=1)
        rows = pl.ds(pl.multiple_of(chunk * 512, 512), 512)
        product = dot(both, wm[rows, :])
        if first:
            acc_p[b] = product
        else:
            acc_p[b] += product

    def take_slot(phase, s, relay):
        for d in range(2):
            z_arrival(phase, d, s).wait_recv()
            if relay:
                z_copy(phase, d, s + BLOCKS).start()

    def add_one(phase, d, s):
        chunk = chunk_at(d, lax.div(s, BLOCKS) + 1)
        if phase == 0:
            add_tokens(chunk, slot_block(d, s))
        else:
            add_passages(chunk, slot_block(d, s))

    hand_groups = (
        ((0, 2), (2, 2), (4, 2), (6, 2), (8, 2), (10, 2), (12, 2)),
        ((0, 2), (2, 2), (4, 2), (6, 2), (8, 2), (10, 2), (12, 1), (13, 1)),
    )

    def take(phase, s):
        take_slot(phase, jnp.int32(s), s < SLOTS - BLOCKS)
        for first, count in hand_groups[phase]:
            if s == first + count - 1:
                for d in range(2):
                    hand_copy(phase, d, first, core, count).start()

    def add(phase, *slots):
        for s in slots:
            for d in range(2):
                for first, count in hand_groups[phase]:
                    if s == first:
                        hand_copy(phase, d, first, other, count).wait_recv()
                add_one(phase, d, jnp.int32(s))

    def add_own(phase):
        hand_copy(phase, 0, -BLOCKS, other, BLOCKS).wait_recv()
        for b in range(BLOCKS):
            if phase == 0:
                add_tokens(z, b, first=True)
            else:
                add_passages(z, b, first=True)

    late = jnp.minimum(row, 2) + jnp.minimum(column, 2) >= 2
    soon = jnp.logical_not(late)

    def greet(ring):
        meet(ring)
        if ring + 1 < len(RINGS):
            tell(ring + 1)
        send_ids(ring)

    def gather_all():
        for ring in range(len(RINGS)):
            gather_rows(ring)

    def send_all():
        for ring in range(len(RINGS)):
            send_rows(ring)

    local_copies[0].wait()
    greet(0)

    @pl.when(late)
    def _():
        greet(1)
        greet(2)
        greet(3)

    take(0, 0)

    @pl.when(soon)
    def _():
        greet(1)

    take(0, 1)

    @pl.when(soon)
    def _():
        greet(2)

    local_copies[1].wait()
    inbox[st] = store_v[wanted_row(lambda pick, b: ids[pick, b])]
    take(0, 2)

    @pl.when(soon)
    def _():
        greet(3)

    take(0, 3)
    pl.when(late)(gather_all)
    take(0, 4)
    pl.when(late)(send_all)
    take(0, 5)
    pl.when(soon)(gather_all)
    for copy in local_copies[2:]:
        copy.wait()
    for chunk in range(RING):
        wg_f[chunk] = wg_v[:, chunk * 512 : (chunk + 1) * 512].astype(F32)
    add_own(0)
    take(0, 6)
    pl.when(soon)(send_all)
    add(0, 0, 1)
    take(0, 7)
    add(0, 2, 3)
    take(0, 8)
    add(0, 4, 5)
    take(0, 9)
    for place in range(N_ST - 1):
        row_copy(place, source(place)).wait_recv()
    for b in range(BLOCKS):
        for pick in range(PICKS):
            owner = lax.shift_right_logical(ids[pick, b], PASS_SHIFT)
            x[1, z, core, b, pick * PASS_ROWS : (pick + 1) * PASS_ROWS, :] = inbox[owner]

    add(0, 6)
    send_own(1)
    add(0, 7)
    take(0, 10)
    take(0, 11)
    take(0, 12)
    add(0, 8, 9)
    take(0, 13)
    add(0, 10, 11)

    rate = decay[0]

    def finish_tokens(b):
        mean_square = jnp.sum(squares[b], axis=1, keepdims=True) * (1.0 / D)
        scale = lax.rsqrt(mean_square + norm_eps)
        cosine = cos_v[b * BLOCK : (b + 1) * BLOCK, :]
        sine = sin_v[b * BLOCK : (b + 1) * BLOCK, :]

        def rotate(values):
            return values * cosine + pltpu.roll(values, KEY_DIM // 2, 1) * sine

        query = rotate(acc[b, :, 0:128] * scale).astype(BF16)
        key = (rotate(acc[b, :, 128:256] * scale) * KEY_DIM ** (-0.5)).astype(BF16)
        key_v[b * BLOCK : (b + 1) * BLOCK, :] = key
        value_v[b * BLOCK : (b + 1) * BLOCK, :] = (acc[b, :, 256:512] * scale).astype(BF16)
        memory = acc[b, :, 512:640]
        mean = jnp.mean(memory * memory, axis=1, keepdims=True)
        mem_q[b] = (memory * lax.rsqrt(mean + norm_eps)).astype(BF16)
        gate = jnp.sum(gates[b], axis=1, keepdims=True) * scale
        gate_v[b] = jnp.broadcast_to(jax.nn.sigmoid(gate), (BLOCK, 128))

        span = (b + 1) * BLOCK
        keys = key_v[0:span, :]
        values = value_v[0:span, :]
        row = lax.broadcasted_iota(jnp.int32, (BLOCK, span), 0) + b * BLOCK
        column = lax.broadcasted_iota(jnp.int32, (BLOCK, span), 1)
        distance = (row - column).astype(F32)
        mask = jnp.where(distance >= 0.0, jnp.exp(-rate * jnp.maximum(distance, 0.0)), 0.0)
        scores = dot_t(query, keys) * mask
        upper = scores.astype(BF16)
        lower = (scores - upper.astype(F32)).astype(BF16)
        mixed = dot(upper, values) + dot(lower, values)
        centred = mixed - jnp.mean(mixed, axis=1, keepdims=True)
        variance = jnp.mean(centred * centred, axis=1, keepdims=True)
        ret_norm[b] = centred * lax.rsqrt(variance + norm_eps)

    def finish_block(b):
        raw = acc_p[b, :, 0:128]
        mean = jnp.mean(raw * raw, axis=1, keepdims=True)
        pass_key = (raw * lax.rsqrt(mean + norm_eps)).astype(BF16)
        lifted = dot(acc_p[b, :, 128:256].astype(BF16), wl_v[0]).astype(BF16)
        exponent = jnp.exp(dot_t(mem_q[b], pass_key) * MEM_DIM ** (-0.5))
        mass = jnp.sum(exponent, axis=1, keepdims=True)
        gate = gate_v[b] / mass
        gate = jnp.concatenate([gate, gate], axis=1)
        lift = dot(exponent.astype(BF16), lifted)
        out[b * BLOCK : (b + 1) * BLOCK, :] = (ret_norm[b] + gate * lift).astype(BF16)

    def hand_done(phase):
        hand_copy(phase, 0, -BLOCKS, core, BLOCKS).wait_send()
        for d in range(2):
            for first, count in hand_groups[phase]:
                hand_copy(phase, d, first, core, count).wait_send()

    for step in range(SLOTS):
        take(1, step)
        if step == 0:
            add(0, 12, 13)
            add_own(1)
        if step % 2 == 0 and step > 0:
            add(1, step - 2, step - 1)
        if step in (1, 3, 5, 7):
            finish_tokens(step // 2)
        if step == 9:

            @pl.loop(0, SLOTS)
            def _(n):
                z_copy(0, 0, n).wait_send()
                z_copy(0, 1, n).wait_send()

            hand_done(0)
            for place in range(N_ST - 1):
                id_copy(place, st).wait_send()
                row_copy(place, st).wait_send()

    add(1, 12)
    finish_block(0)
    finish_block(2)
    add(1, 13)
    finish_block(1)
    finish_block(3)

    @pl.loop(0, SLOTS)
    def _(n):
        z_copy(1, 0, n).wait_send()
        z_copy(1, 1, n).wait_send()

    hand_done(1)


def per_device(
    tokens,
    w_query,
    w_key,
    w_value,
    w_mem_query,
    w_mem_key,
    w_mem_value,
    w_gate,
    w_lift,
    decay_rate,
    store,
    passage_ids,
):
    cos_table, sin_table = rotary_tables()
    hbm = pl.BlockSpec(memory_space=pltpu.HBM)
    dma = pltpu.SemaphoreType.DMA
    operands = (
        tokens,
        w_query,
        w_key,
        w_value,
        w_mem_query,
        w_mem_key,
        w_mem_value,
        w_gate.reshape(1, D),
        w_lift,
        store,
        jnp.asarray(cos_table),
        jnp.asarray(sin_table),
        passage_ids.T,
    )
    return pl.pallas_call(
        kernel,
        out_shape=pltpu.VMEM((SEQ_LEN, VALUE_DIM), BF16),
        in_specs=[pl.BlockSpec(memory_space=pltpu.SMEM)] + [hbm] * 13,
        out_specs=pl.BlockSpec(memory_space=pltpu.VMEM),
        scratch_shapes=[
            pltpu.VMEM((2, RING, 2, BLOCKS, BLOCK, HALF), BF16),
            pltpu.VMEM((D, TOK_COLS), BF16),
            pltpu.VMEM((D, 2 * MEM_DIM), BF16),
            pltpu.VMEM(store.shape, BF16),
            pltpu.VMEM((N_ST, PASS_ROWS, HALF), BF16),
            pltpu.VMEM((N_ST, PASS_ROWS, HALF), BF16),
            pltpu.VMEM((BLOCKS, BLOCK, TOK_COLS), F32),
            pltpu.VMEM((BLOCKS, BLOCK, 128), F32),
            pltpu.VMEM((BLOCKS, BLOCK, 128), F32),
            pltpu.VMEM((BLOCKS, BLOCK, 2 * MEM_DIM), F32),
            pltpu.VMEM((SEQ_LEN, KEY_DIM), BF16),
            pltpu.VMEM((SEQ_LEN, VALUE_DIM), BF16),
            pltpu.VMEM((BLOCKS, BLOCK, MEM_DIM), BF16),
            pltpu.VMEM((BLOCKS, BLOCK, 128), F32),
            pltpu.VMEM((BLOCKS, BLOCK, VALUE_DIM), F32),
            pltpu.VMEM((1, D), BF16),
            pltpu.VMEM((RING, 1, 512), F32),
            pltpu.VMEM((1, MEM_DIM, VALUE_DIM), BF16),
            pltpu.VMEM((SEQ_LEN, KEY_DIM), F32),
            pltpu.VMEM((SEQ_LEN, KEY_DIM), F32),
            pltpu.SMEM((PICKS, BLOCKS), jnp.int32),
            pltpu.SMEM((N_ST, PICKS, BLOCKS), jnp.int32),
            dma((BLOCKS,)),
            dma((12,)),
            dma((2, 2, SLOTS)),
            dma((2, 2, SLOTS)),
            dma((2, 2, BLOCKS + SLOTS)),
            dma((2, 2, BLOCKS + SLOTS)),
            dma((N_ST,)),
            dma((N_ST,)),
            dma((N_ST,)),
            dma((N_ST,)),
            pltpu.SemaphoreType.REGULAR((4,)),
        ],
        compiler_params=pltpu.CompilerParams(
            collective_id=0, has_side_effects=True, vmem_limit_bytes=48 * 1024 * 1024
        ),
        name="fused_layer",
    )(decay_rate, *[pltpu.with_memory_space_constraint(array, pltpu.HBM) for array in operands])


def solution(mesh):
    in_specs = (
        P("st", "tp"),
        P(None, "tp"),
        P(None, "tp"),
        P(None, "tp"),
        P(None, "tp"),
        P(None, "tp"),
        P(None, "tp"),
        P(None, "tp"),
        P("tp", None, None),
        P("tp"),
        P("st", None, "tp"),
        P("st", None),
    )
    out_specs = P("st", "tp")
    return jax.shard_map(
        per_device, mesh=mesh, in_specs=in_specs, out_specs=out_specs, check_vma=False
    )
```
